32 devices in a mesh: grp: 2 (over y), sp: 4 (over z), tp: 4 (over x, core).
Axes of the slice: x: 2, y: 2, z: 4, core: 2. Of those that a mesh axis runs over, the one named last changes fastest.
Arguments:
- resid: bfloat16 [4096, 2048], P(('grp', 'sp', 'tp')), parts along dimension 0, may hold values from -6 to 6
- pool_input: bfloat16 [4096, 512], P(('grp', 'sp'), 'tp'), parts along dimension 0, may hold values from -6 to 6
- group_map: bfloat16 [4, 128, 128], P('tp'), may hold values from -0.5 to 0.5
- pool_scale: bfloat16 [512], P('tp'), may hold values from 0.099609375 to 1.8984375
- out_proj: bfloat16 [512, 2048], P('tp'), may hold values from -0.25 to 0.25
- norm_gain: bfloat16 [2048], replicated, may hold values from 0.099609375 to 1.8984375
- routes: int32 [4096, 2], P(('grp', 'sp', 'tp')), parts along dimension 0, may hold values from 0 to 3, all different within a row; in each aligned block of 128 rows (0 to 127, 128 to 255, ...) at most 80 rows name the same one
- route_weight: float32 [4096, 2], P(('grp', 'sp', 'tp')), parts along dimension 0, may hold values from 0.2 to 1
- expert_gate: bfloat16 [4, 2048, 3584], P('sp', None, 'tp'), may hold values from -0.125 to 0.125
- expert_up: bfloat16 [4, 2048, 3584], P('sp', None, 'tp'), may hold values from -0.125 to 0.125
- expert_down: bfloat16 [4, 3584, 2048], P('sp', 'tp'), may hold values from -0.09375 to 0.09375
Outputs:
- layer_out: bfloat16 [4096, 2048], P(('grp', 'sp', 'tp')), parts along dimension 0
The draws below stay inside these ranges and needn't reach their ends.
There are 2 independent parts, one for each index of `grp`. The reference program is written for one: setup_inputs(seed, part) draws one part's arguments, and reference() takes and returns one part's arrays. A program takes and returns all parts, laid end to end along the dimension named above; an argument that names none is the same for every part. Nothing has to cross between parts.
Inputs may be any that keep to these rules, and one draw needn't show every extreme that they name: The 2 routes of a token differ. Among the tokens of one device (aligned blocks of 128 tokens), no expert is named more than 80 times, and in every draw some device names some expert exactly 80 times.
All inputs are finite; a program needn't handle non-finite values.
Results may differ from the reference program's by a relative error of at most 0.011.
Values may be sent and summed in bfloat16 or wider, within the bound.
A program may use at most 128 MiB of HBM per device.

```python
import math
import jax
import jax.numpy as jnp
import numpy as np
from jax import lax

D = 2048
GROUPS = 4
POOL_WIDTH = 512
GROUP_DIM = 128
EXPERT_FF = 3584
TOPK = 2
EXPERTS = 4
ROWS_DEV = 128
TOKENS = 2048
CAP = 80
N_SP = 4
N_TP = 4


def levels(key, dims, split, low, top_value):
    loudness = 1.0
    for position, blocks in split:
        steps = jax.random.uniform(jax.random.fold_in(jax.random.fold_in(key, 6), position), (blocks,), jnp.float32, low / len(split), top_value / len(split))
        loudness = loudness * jnp.repeat(jnp.exp(steps), dims[position] // blocks).reshape((-1,) + (1,) * (len(dims) - 1 - position))
    return loudness


def deal_out(own_key, own, number, rows, count, top, most, lean):
    sequence = jax.random.permutation(own_key, count)
    crowded, common = portions_of(count, rows * top, most, lean, True), portions_of(count, rows * top, most, lean, False)
    places = jnp.arange(count)

    def named(sizes, rotation):
        used = int((sizes > 0).sum())
        fixed = max(1, used // 4)
        shifted = fixed + (places - fixed + rotation * (used - fixed)) % max(1, count - fixed)
        return jnp.zeros((count,), jnp.int32).at[sequence[jnp.where(places < fixed, places, shifted)]].set(jnp.asarray(sizes, jnp.int32))

    sizes = jnp.where(number % 4 == 0, named(crowded, number // 4), named(common, number - number // 4 - 1))
    mixed = jax.random.permutation(jax.random.fold_in(own, 3), count)
    source_of, taker = mixed[0:count // 2 * 2:2], mixed[1:count // 2 * 2:2]
    slack = jnp.minimum(sizes[source_of] - 1, most - sizes[taker]) // 2
    slack = jnp.where((source_of == sequence[0]) | (taker == sequence[0]) | (sizes[taker] == 0), 0, jnp.maximum(slack, 0))
    shifted = jax.random.randint(jax.random.fold_in(own, 4), (count // 2,), 0, 1 << 20) % (slack + 1)
    sizes = sizes.at[source_of].add(-shifted).at[taker].add(shifted)
    members = jnp.searchsorted(jnp.cumsum(sizes), jnp.arange(rows * top), side="right").astype(jnp.int32)
    grid = members.reshape(top, rows).T
    grid = grid[jax.random.permutation(jax.random.fold_in(own, 1), rows)]
    rotation = jax.random.randint(jax.random.fold_in(own, 2), (rows, 1), 0, top)
    return jnp.take_along_axis(grid, (jnp.arange(top)[None, :] + rotation) % top, axis=1)


def portions_of(amount, total, reach, lean, full):
    portions = [(1 << 20) // math.isqrt(grade ** lean) + 1 for grade in range(1, amount + 1)]
    largest = reach if full else min(reach, max(-(-total // amount), total * portions[0] // sum(portions)))
    least = 1 if total - largest >= amount - 1 else 0
    counts, rest = [largest] + [least] * (amount - 1), total - largest - least * (amount - 1)
    while rest > 0:
        candidates = [i for i in range(1, amount) if counts[i] < largest] or [i for i in range(1, amount) if counts[i] < reach]
        mass, remaining = sum([portions[i] for i in candidates]), rest
        for i in candidates:
            more = min(reach - counts[i], max(1, remaining * portions[i] // mass), rest)
            counts[i] = counts[i] + more
            rest = rest - more
    return np.array(counts)


def bell_draw(key, shape, spread, limit, cuts=(), kind=jnp.bfloat16):
    result = spread * jax.random.normal(key, shape, jnp.float32)
    if cuts:
        result = result * levels(key, shape, cuts, -0.22, 0.18)
    return jnp.clip(result, -limit, limit).astype(kind)


def setup_inputs(seed: int = 0, part: int = 0) -> dict:
    keys = jax.random.split(jax.random.key(seed), 12)
    part_splits = jax.random.split(jax.random.fold_in(keys[11], part), 12)
    resid = bell_draw(part_splits[0], (TOKENS, D), 1.0, 6.0, ((0, 16),))
    pool_input = bell_draw(part_splits[1], (TOKENS, POOL_WIDTH), 1.0, 6.0, ((0, 4), (1, 4)))
    group_map = bell_draw(keys[2], (GROUPS, GROUP_DIM, GROUP_DIM), GROUP_DIM ** -0.5, 0.5, ((0, 4),))
    pool_scale = jnp.clip(1.0 + 0.18 * jax.random.normal(keys[3], (POOL_WIDTH,), jnp.float32), 0.099609375, 1.8984375).astype(jnp.bfloat16)
    out_proj = bell_draw(keys[4], (POOL_WIDTH, D), POOL_WIDTH ** -0.5, 0.25, ((0, 4),))
    norm_gain = jnp.clip(1.0 + 0.18 * jax.random.normal(keys[5], (D,), jnp.float32), 0.099609375, 1.8984375).astype(jnp.bfloat16)
    routes_keys = jax.random.split(jax.random.fold_in(part_splits[6], 1), TOKENS // ROWS_DEV)
    routes_turns = jax.random.permutation(jax.random.fold_in(part_splits[6], 3), TOKENS // ROWS_DEV)
    routes = jax.vmap(lambda own, number: deal_out(jax.random.fold_in(part_splits[6], 2), own, number, ROWS_DEV, EXPERTS, TOPK, CAP, 1))(routes_keys, routes_turns).reshape((TOKENS, TOPK))
    route_weight = jnp.clip(0.2 + 0.8 * jax.random.uniform(part_splits[7], (TOKENS, TOPK), jnp.float32) ** levels(part_splits[7], (TOKENS, TOPK), ((0, 16),), -0.2, 0.2), 0.2, 1.0)
    expert_gate = bell_draw(keys[8], (EXPERTS, D, EXPERT_FF), D ** -0.5, 0.125, ((0, 4), (2, 4)))
    expert_up = bell_draw(keys[9], (EXPERTS, D, EXPERT_FF), D ** -0.5, 0.125, ((0, 4), (2, 4)))
    expert_down = bell_draw(keys[10], (EXPERTS, EXPERT_FF, D), EXPERT_FF ** -0.5, 0.09375, ((0, 4), (1, 4)))
    return {"resid": resid, "pool_input": pool_input, "group_map": group_map, "pool_scale": pool_scale, "out_proj": out_proj, "norm_gain": norm_gain, "routes": routes, "route_weight": route_weight, "expert_gate": expert_gate, "expert_up": expert_up, "expert_down": expert_down}


norm_eps = 1e-06

def pool_group(values, window):
    window_sum = values
    for back in range(1, window):
        window_sum = window_sum + jnp.pad(values[:-back], ((back, 0), (0, 0)))
    divisor = jnp.minimum(jnp.arange(1, values.shape[0] + 1, dtype=jnp.float32), jnp.float32(window))
    return (window_sum / divisor[:, None] - values).astype(jnp.bfloat16)

def reference(resid, pool_input, group_map, pool_scale, out_proj, norm_gain, routes, route_weight, expert_gate, expert_up, expert_down):
    values = pool_input.astype(jnp.float32)
    pieces = []
    for group in range(GROUPS):
        low = group * GROUP_DIM
        pooled = pool_group(values[:, low:low + GROUP_DIM], 2 ** (group + 1))
        product = jnp.dot(pooled, group_map[group], preferred_element_type=jnp.float32)
        pieces.append((product * pool_scale[low:low + GROUP_DIM].astype(jnp.float32)).astype(jnp.bfloat16))
    group_out = jnp.concatenate(pieces, axis=1)
    mix = jnp.dot(group_out, out_proj, preferred_element_type=jnp.float32)
    mixed = (resid.astype(jnp.float32) + mix).astype(jnp.bfloat16)
    residual = mixed.astype(jnp.float32)
    scaled = residual * lax.rsqrt(lax.optimization_barrier(jnp.mean(residual * residual, axis=1, keepdims=True)) + norm_eps)
    normed = (scaled * norm_gain.astype(jnp.float32)).astype(jnp.bfloat16)
    flat_routes = routes.reshape(-1).astype(jnp.int32)
    flat_rows = jnp.repeat(normed, TOPK, axis=0)
    buffer_rows = N_SP * N_TP * CAP
    quarter = EXPERT_FF // N_TP

    def per_expert(carry, expert):
        chosen = flat_routes == expert
        rank = (jnp.cumsum(chosen.astype(jnp.int32)) - 1).astype(jnp.int32)
        place = jnp.where(chosen, rank, buffer_rows).astype(jnp.int32)
        buffer = jnp.zeros((buffer_rows, D), jnp.bfloat16).at[place].set(flat_rows, mode='drop')
        gate = jnp.dot(buffer, expert_gate[expert], preferred_element_type=jnp.float32)
        up_value = jnp.dot(buffer, expert_up[expert], preferred_element_type=jnp.float32)
        hidden = (jax.nn.silu(gate) * up_value).astype(jnp.bfloat16)
        down_w = expert_down[expert]
        output = jnp.zeros((buffer_rows, D), jnp.float32)
        for lane in range(N_TP):
            partial_out = jnp.dot(hidden[:, lane * quarter:(lane + 1) * quarter], down_w[lane * quarter:(lane + 1) * quarter], preferred_element_type=jnp.float32)
            output = output + lax.optimization_barrier(partial_out.astype(jnp.bfloat16)).astype(jnp.float32)
        picked = jnp.take(output, jnp.minimum(place, buffer_rows - 1), axis=0)
        return (carry + jnp.where(chosen[:, None], picked, jnp.float32(0.0)), None)
    routed, _ = lax.scan(per_expert, jnp.zeros((TOKENS * TOPK, D), jnp.float32), jnp.arange(EXPERTS, dtype=jnp.int32))
    moe = lax.optimization_barrier(jnp.sum(routed.reshape(TOKENS, TOPK, D) * route_weight.astype(jnp.float32)[:, :, None], axis=1))
    return (residual + moe).astype(jnp.bfloat16)
```

```python
import functools

import jax
import jax.numpy as jnp
from jax import lax
from jax.experimental import pallas as pl
from jax.experimental.pallas import tpu as pltpu
from jax.sharding import PartitionSpec as P

GROUPS = 4
norm_eps = 1e-06
BF = jnp.bfloat16
F32 = jnp.float32
MESH = pl.DeviceIdType.MESH
RIM = 2**GROUPS
ORDER = ((0, 1, 2, 3), (1, 3, 0, 2), (2, 0, 3, 1), (3, 2, 1, 0))
SENDS = ((0, 2, 1, 3), (1, 3, 0, 2), (2, 0, 3, 1), (3, 1, 2, 0))


def nearest(s, j, S):
    low = jnp.minimum(s, S - 1 - s)
    half = (j + 1) // 2
    both = half * (2 * lax.rem(j, 2) - 1)
    rest = (j - low) * (1 - 2 * ((2 * s) // S))
    return s + jnp.where(j <= 2 * low, both * (1 - 2 * ((2 * s) // S)), rest)


def look_up(table, s, j):
    value = 0
    for a, row in enumerate(table):
        for b, entry in enumerate(row):
            value = value + jnp.where((s == a) & (j == b), entry, 0)
    return value


def visit(s, j, S):
    return look_up(ORDER, s, j) if S == 4 else nearest(s, lax.rem(S - j, S), S)


def sends(s, j, S):
    return look_up(SENDS, s, j) if S == 4 else nearest(s, S - j, S)


def kernel(
    G, S, T, R, SL, NC,
    resid, pool, gmap, scale, oproj, gain, routes_t, weight_t, wg, wu, wd,
    out,
    wgu_v, wd_v, opj, rim, piece, gout, stage, inbox, pbuf, rbuf, fbuf, fin, ret,
    acc, hid, mixed_v, cast_v, rsend, rin,
    w_sem, ox_s, ox_r, oy_s, oy_r, on_s, on_r, rim_s, rim_r, pc_s, pc_r,
    z_s, z_r, f_s, f_r, n_s, n_r, pn_s, pn_r, pf_s, pf_r, rz_s, rz_r, rr_s, rr_r,
):
    g = lax.axis_index("grp")
    s = lax.axis_index("sp")
    t = lax.axis_index("tp")
    H = T // 2
    D = resid.shape[1]
    F = wd.shape[0]
    DC = D // NC
    GD = oproj.shape[0]
    GH = GD // G
    C = range(NC)
    near = t + 1 - 2 * lax.rem(t, 2)
    inner = (s != 0) & (s != S - 1)

    def cut(c):
        return slice(c * DC, (c + 1) * DC)

    def up(k):
        return lax.rem(t + 2 * k, T)

    def down(base, k):
        return lax.rem(base - 2 * k + 2 * T, T)

    def remote(src, dst, ss, rs, sp=None, tp=None, grp=None):
        return pltpu.make_async_remote_copy(
            src_ref=src, dst_ref=dst, send_sem=ss, recv_sem=rs,
            device_id={
                "grp": g if grp is None else grp,
                "sp": s if sp is None else sp,
                "tp": t if tp is None else tp,
            },
            device_id_type=MESH,
        )

    loads = [
        pltpu.make_async_copy(wg, wgu_v.at[:, pl.ds(0, F)], w_sem.at[0]),
        pltpu.make_async_copy(wu, wgu_v.at[:, pl.ds(F, F)], w_sem.at[1]),
        pltpu.make_async_copy(wd, wd_v, w_sem.at[2]),
    ]
    for load in loads:
        load.start()

    barrier = pltpu.get_barrier_semaphore()

    @pl.loop(1, S * T)
    def _(j):
        peer = lax.rem(s * T + t + j, S * T)
        pl.semaphore_signal(
            barrier, inc=1, device_id={"grp": g, "sp": peer // T, "tp": lax.rem(peer, T)},
            device_id_type=MESH,
        )

    for j in range(1, G):
        pl.semaphore_signal(
            barrier, inc=1, device_id={"grp": lax.rem(g + j, G), "sp": s, "tp": t},
            device_id_type=MESH,
        )
    pl.semaphore_wait(barrier, S * T - 1 + G - 1)

    seq = pool.shape[0]
    rim_copy = remote(
        pool.at[pl.ds(seq - RIM, RIM)], rim, rim_s.at[0], rim_r.at[0], sp=lax.rem(s + 1, S)
    )
    rim_copy.start()

    def own_rows(h):
        return pl.ds(pl.multiple_of(h * GH, GH), GH)

    def o_far(k, c):
        return remote(
            oproj.at[own_rows(g), cut(c)], opj.at[c, t, own_rows(g)],
            ox_s.at[k, c], ox_r.at[k, c], tp=up(k),
        )

    def o_part(k, j, c):
        part = opj.at[c, down(t, k), own_rows(g)]
        return remote(part, part, oy_s.at[k, j, c], oy_r.at[k, j, c], grp=lax.rem(g + j, G))

    def o_near(k, c):
        block = opj.at[c, down(t, k)]
        return remote(
            oproj.at[:, cut(c)] if k == 0 else block, block, on_s.at[k, c], on_r.at[k, c], tp=near
        )

    def o_spread(c):
        for k in range(1, H):
            o_far(k, c).wait_recv()
            for j in range(1, G):
                o_part(k, j, c).start()

    def o_pass(c):
        for k in range(1, H):
            for j in range(1, G):
                o_part(k, j, c).wait_recv()
            o_near(k, c).start()

    for c in range(NC - 1):
        for k in range(1, H):
            o_far(k, c).start()
    for c in C:
        o_near(0, c).start()

    E = S
    EP = max(8, E)
    e_row = lax.broadcasted_iota(jnp.int32, (EP, R), 0)
    hot_row = [e_row == routes_t[k : k + 1, :] for k in range(2)]
    both_row = jnp.where(hot_row[0] | hot_row[1], 1.0, 0.0).astype(BF)
    before = lax.broadcasted_iota(jnp.int32, (R, R), 0) < lax.broadcasted_iota(
        jnp.int32, (R, R), 1
    )
    rank_row = jnp.dot(both_row, jnp.where(before, 1.0, 0.0).astype(BF), preferred_element_type=F32)
    slot_row = rank_row + (e_row * SL).astype(F32)
    tgt_row = [jnp.sum(jnp.where(h, slot_row, 0.0), axis=0, keepdims=True) for h in hot_row]

    eye = lax.broadcasted_iota(jnp.int32, (R, R), 0) == lax.broadcasted_iota(
        jnp.int32, (R, R), 1
    )

    def column(row):
        return jnp.sum(jnp.where(eye, row, 0.0), axis=1, keepdims=True)

    tgt_col = [column(row) for row in tgt_row]
    weight_col = [column(weight_t[k : k + 1, :]) for k in range(2)]

    rim_copy.wait_recv()
    values = pool[...].astype(F32)
    rim_v = jnp.where(s > 0, rim[...].astype(F32), 0.0)
    run = jnp.concatenate([rim_v, values], axis=0)
    window_sum = None
    for n in range(GROUPS):
        run = run + pltpu.roll(run, 2**n, 0)
        part = run[RIM:]
        window_sum = part if n == 0 else jnp.where(t >= n, part, window_sum)
    window = jnp.int32(2)
    for n in range(1, GROUPS):
        window = jnp.where(t >= n, jnp.int32(2 ** (n + 1)), window)
    position = s * seq + 1 + lax.broadcasted_iota(jnp.int32, (seq, GD), 0)
    divisor = jnp.minimum(position, window).astype(F32)
    pooled = (window_sum / divisor - values).astype(BF)
    product = jnp.dot(pooled, gmap[0], preferred_element_type=F32)
    piece[...] = (product * scale[...].astype(F32)).astype(BF).reshape(T, R, GD)

    def piece_copy(j):
        q = lax.rem(t + j, T)
        return remote(piece.at[q], gout.at[t], pc_s.at[j], pc_r.at[j], tp=q)

    for j in range(1, T):
        piece_copy(j).start()
    for k in range(1, H):
        o_far(k, NC - 1).start()
    gout[t] = piece[t]
    for c in C:
        opj[c, t] = oproj[:, cut(c)]

    slots = S * SL
    slot_iota = lax.broadcasted_iota(jnp.int32, (slots, R), 0).astype(F32)
    place = jnp.where((tgt_row[0] == slot_iota) | (tgt_row[1] == slot_iota), 1.0, 0.0).astype(BF)

    def z_copy(e, c):
        return remote(stage.at[c, e], inbox.at[s, c, t], z_s.at[e, c], z_r.at[s, c], sp=e)

    def z_arrival(i, c):
        return remote(stage.at[c, i], inbox.at[i, c, t], z_s.at[i, c], z_r.at[i, c], sp=i)

    def far_copy(i, k, c):
        block = inbox.at[i, c, t]
        return remote(block, block, f_s.at[i, k, c], f_r.at[i, k, c], tp=up(k))

    def near_copy(i, k, c):
        block = inbox.at[i, c, down(t, k)]
        return remote(block, block, n_s.at[i, k, c], n_r.at[i, k, c], tp=near)

    def r_copy(e, q):
        return remote(rsend.at[e], rin.at[s, t], rr_s.at[e, q], rr_r.at[s, t], sp=e, tp=q)

    def r_arrival(i, q):
        return remote(rsend.at[i], rin.at[i, q], rr_s.at[i, q], rr_r.at[i, q], sp=i, tp=q)

    def p_near(i, k, c):
        return remote(
            pbuf.at[i, c, down(near, k)], rbuf.at[i, k, c], pn_s.at[i, k, c], pn_r.at[i, k, c],
            tp=near,
        )

    def p_far(i, k, c):
        q = down(t, k)
        return remote(pbuf.at[i, c, q], fbuf.at[i, k, c], pf_s.at[i, k, c], pf_r.at[i, k, c], tp=q)

    def back(i, c):
        return remote(fin.at[i, c], ret.at[c, s], rz_s.at[i, c], rz_r.at[s, c], sp=i)

    def back_arrival(e, c):
        return remote(fin.at[e, c], ret.at[c, e], rz_s.at[e, c], rz_r.at[e, c], sp=e)

    def push(i, c):
        for k in range(1, H):
            far_copy(i, k, c).start()
        near_copy(i, 0, c).start()

    def fwd(p, c):
        i = visit(s, p, S)
        z_arrival(i, c).wait_recv()
        push(i, c)

    def relay(p, c):
        i = visit(s, p, S)
        for k in range(1, H):
            far_copy(i, k, c).wait_recv()
            near_copy(i, k, c).start()

    def ready(p):
        i = visit(s, p, S)
        for c in C:
            for k in range(H):
                near_copy(i, k, c).wait_recv()

        @pl.loop(0, T)
        def _(q):
            @pl.when((i != s) | (q != t))
            def _():
                r_arrival(i, q).wait_recv()

    NT = 256 if (2 * F) % 256 == 0 else 128
    DT = 512
    GN = 2 * F // NT

    def hidden(p, lo, hi):
        i = visit(s, p, S)

        def one(n):
            cols = pl.ds(pl.multiple_of(n * NT, NT), NT)
            total = None
            for c in C:
                x = inbox[i, c].reshape(T * SL, DC)
                y = jnp.dot(x, wgu_v[cut(c), cols], preferred_element_type=F32)
                total = y if total is None else total + y
            acc[:, cols] = total

        for n in range(lo, hi):
            one(n)

    def gated(p):
        i = visit(s, p, S)
        spot = lax.broadcasted_iota(jnp.int32, (SL, 128), 0) == lax.broadcasted_iota(
            jnp.int32, (SL, 128), 1
        )
        for q in range(T):
            rows = slice(q * SL, (q + 1) * SL)
            r = jnp.sum(jnp.where(spot, rin[i, q], 0.0), axis=1, keepdims=True)
            gate = acc[rows, :F] * r
            hid[rows] = (gate / (1.0 + jnp.exp(-gate)) * (acc[rows, F:] * r)).astype(BF)

    def lower(p, c):
        i = visit(s, p, S)

        for n in range(DC // DT):
            y = jnp.dot(
                hid[...], wd_v[:, c * DC + n * DT : c * DC + (n + 1) * DT],
                preferred_element_type=F32,
            )
            pbuf[i, c, :, :, n * DT : (n + 1) * DT] = y.astype(BF).reshape(T, SL, DT)

        for k in range(H):
            p_near(i, k, c).start()

    def pair(p, c):
        i = visit(s, p, S)
        for k in range(H):
            p_near(i, k, c).wait_recv()
        for k in range(1, H):
            q = down(t, k)
            pbuf[i, c, q] = (pbuf[i, c, q].astype(F32) + rbuf[i, k, c].astype(F32)).astype(BF)
            p_far(i, k, c).start()

    def finish(p, c):
        i = visit(s, p, S)
        value = pbuf[i, c, t].astype(F32) + rbuf[i, 0, c].astype(F32)
        for k in range(1, H):
            p_far(i, k, c).wait_recv()
            value = value + fbuf[i, k, c].astype(F32)
        return i, value.astype(BF)

    def send_back(p, c):
        i, value = finish(p, c)
        fin[i, c] = value
        back(i, c).start()

    def only(where, act, p, *c):
        @pl.when(where)
        def _():
            for n in c:
                act(p, n)

    def mix_part(c, wide, square):
        for k in range(H):
            o_near(k, c).wait_recv()
        total = jnp.dot(wide, opj[c].reshape(T * GD, DC), preferred_element_type=F32)
        mixed = (resid[:, cut(c)].astype(F32) + total).astype(BF)
        mixed_v[:, cut(c)] = mixed
        residual = mixed.astype(F32)
        cast = (residual * gain[cut(c)].astype(F32).reshape(1, DC)).astype(BF)
        stage[c] = jnp.dot(place, cast, preferred_element_type=F32).astype(BF).reshape(S, SL, DC)
        inbox[s, c, t] = stage[c, s]

        z_copy(sends(s, 1, S), c).start()

        @pl.when(inner)
        def _():
            z_copy(sends(s, 2, S), c).start()

        push(s, c)
        return square + jnp.sum(residual * residual, axis=1, keepdims=True)

    square = jnp.zeros((R, 1), F32)
    o_spread(0)
    o_spread(1)
    for c in range(2, NC):
        o_pass(c - 2)
        o_spread(c)
    for j in range(1, T):
        piece_copy(j).wait_recv()
    wide = jnp.concatenate([gout[q] for q in range(T)], axis=1)
    for c in C:
        square = mix_part(c, wide, square)
        if c + 2 < NC:
            o_pass(c + NC - 2)
    unit = lax.rsqrt(square * (1.0 / D) + norm_eps)

    @pl.loop(0, S)
    def _(e):
        lane = (lax.broadcasted_iota(jnp.int32, (R, 128), 1) + e * SL).astype(F32)
        inside = lax.broadcasted_iota(jnp.int32, (R, 128), 1) < SL
        mine = ((tgt_col[0] == lane) | (tgt_col[1] == lane)) & inside
        rsend[e] = jnp.sum(jnp.where(mine, unit, 0.0), axis=0, keepdims=True)

    rin[s, t] = rsend[s]

    @pl.loop(1, S * T)
    def _(j):
        peer = lax.rem(s * T + t + j, S * T)
        r_copy(peer // T, lax.rem(peer, T)).start()

    @pl.loop(jnp.where(inner, 3, 2), S)
    def _(j):
        for c in C:
            z_copy(sends(s, j, S), c).start()

    for load in loads:
        load.wait()

    if S == 4:
        edge = (s == 0) | (s == S - 1)
        relay(0, 0)
        fwd(1, 0)
        relay(0, 1)
        fwd(1, 1)
        relay(0, 2)
        fwd(1, 2)
        relay(0, 3)
        ready(0)
        hidden(0, 0, 3)
        fwd(1, 3)
        relay(1, 0)
        hidden(0, 3, 5)
        relay(1, 1)
        hidden(0, 5, 7)
        fwd(2, 0)
        gated(0)
        lower(0, 0)
        relay(1, 2)
        lower(0, 1)
        fwd(2, 1)
        lower(0, 2)
        lower(0, 3)
        fwd(2, 2)
        relay(1, 3)
        ready(1)
        hidden(1, 0, 3)
        fwd(2, 3)
        relay(2, 0)
        hidden(1, 3, 5)
        relay(2, 1)
        hidden(1, 5, 7)
        only(edge, fwd, 3, 0)
        relay(2, 2)
        gated(1)
        lower(1, 0)
        only(edge, fwd, 3, 1)
        lower(1, 1)
        lower(1, 2)
        only(inner, pair, 1, 0)
        relay(2, 3)
        lower(1, 3)
        only(inner, pair, 1, 1)
        only(edge, fwd, 3, 2)
        only(inner, pair, 1, 2, 3)
        only(edge, fwd, 3, 3)
        ready(2)
        hidden(2, 0, 3)
        only(inner, send_back, 1, 0)
        only(edge, relay, 3, 0)
        only(inner, fwd, 3, 0)
        hidden(2, 3, 5)
        only(edge, relay, 3, 1)
        only(inner, fwd, 3, 1)
        only(inner, send_back, 1, 1)
        hidden(2, 5, 7)
        gated(2)
        only(edge, relay, 3, 2)
        only(inner, fwd, 3, 2)
        only(inner, send_back, 1, 2)
        lower(2, 0)
        lower(2, 1)
        only(edge, pair, 2, 0)
        lower(2, 2)
        only(edge, pair, 2, 1)
        only(edge, relay, 3, 3)
        only(inner, fwd, 3, 3)
        lower(2, 3)
        only(inner, send_back, 1, 3)
        only(edge, pair, 2, 2, 3)
        only(inner, pair, 2, 0, 1, 2, 3)
        only(inner, relay, 3, 0, 1, 2, 3)
        ready(3)
        hidden(3, 0, 3)
        only(edge, send_back, 2, 0)
        hidden(3, 3, 5)
        only(edge, send_back, 2, 1)
        only(inner, send_back, 2, 0)
        hidden(3, 5, 7)
        gated(3)
        only(edge, send_back, 2, 2)
        only(inner, send_back, 2, 1)
        lower(3, 0)
        lower(3, 1)
        pair(3, 0)
        lower(3, 2)
        pair(3, 1)
        only(inner, send_back, 2, 2)
        lower(3, 3)
        only(edge, send_back, 2, 3)
        pair(3, 2)
        pair(3, 3)
        only(edge, pair, 1, 0, 1, 2, 3)
        pair(0, 0)
        pair(0, 1)
        pair(0, 2)
        pair(0, 3)
        only(inner, send_back, 2, 3)
        send_back(3, 0)
        send_back(3, 1)
        send_back(3, 2)
        send_back(3, 3)
        only(edge, send_back, 1, 0, 1, 2, 3)
    else:
        @pl.loop(0, S + 1)
        def _(j):
            @pl.when(j < S)
            def _():
                for c in C:
                    relay(j, c)

            @pl.when(j + 1 < S)
            def _():
                for c in C:
                    fwd(j + 1, c)

            @pl.when(j > 1)
            def _():
                for c in C:
                    pair(j - 1, c)

            @pl.when(j < S)
            def _():
                ready(j)
                hidden(j, 0, GN)
                gated(j)
                for c in C:
                    lower(j, c)

            @pl.when(j > 1)
            def _():
                for c in C:
                    send_back(j - 1, c)

        for c in C:
            pair(0, c)

    lanes = lax.broadcasted_iota(jnp.int32, (R, slots), 1).astype(F32)
    pick = [jnp.where(tgt_col[k] == lanes, 1.0, 0.0).astype(BF) for k in range(2)]

    for c in C:
        _, value = finish(0, c)
        ret[c, s] = value

        @pl.loop(1, S)
        def _(j):
            back_arrival(visit(s, j, S), c).wait_recv()

        flat = ret[c].reshape(slots, DC)
        total = mixed_v[:, cut(c)].astype(F32)
        picked = [
            weight_col[k] * jnp.dot(pick[k], flat, preferred_element_type=F32) for k in range(2)
        ]
        out[:, cut(c)] = (total + (picked[0] + picked[1])).astype(BF)

    rim_copy.wait_send()
    for c in C:
        for k in range(1, H):
            o_far(k, c).wait_send()
            for j in range(1, G):
                o_part(k, j, c).wait_send()
        for k in range(H):
            o_near(k, c).wait_send()
    for j in range(1, T):
        piece_copy(j).wait_send()

    @pl.loop(0, S)
    def _(i):
        for c in C:
            for k in range(1, H):
                far_copy(i, k, c).wait_send()
                p_far(i, k, c).wait_send()
            for k in range(H):
                near_copy(i, k, c).wait_send()
                p_near(i, k, c).wait_send()

    @pl.loop(1, S)
    def _(j):
        i = visit(s, j, S)
        for c in C:
            z_copy(i, c).wait_send()
            back(i, c).wait_send()

    @pl.loop(1, S * T)
    def _(j):
        peer = lax.rem(s * T + t + j, S * T)
        r_copy(peer // T, lax.rem(peer, T)).wait_send()


def local(
    resid, pool_input, group_map, pool_scale, out_proj, norm_gain, routes, route_weight,
    expert_gate, expert_up, expert_down,
):
    G, S, T = lax.axis_size("grp"), lax.axis_size("sp"), lax.axis_size("tp")
    R, D = resid.shape
    H = T // 2
    top = routes.shape[1]
    experts = S * expert_gate.shape[0]
    room = max(2, 5 * R * top // (4 * experts))
    SL = -(-room // 16) * 16
    F = expert_down.shape[1]
    GD = group_map.shape[1]
    NC = 4
    DC = D // NC
    vmem, hbm = pl.BlockSpec(memory_space=pltpu.VMEM), pl.BlockSpec(memory_space=pl.ANY)
    dma = lambda *n: pltpu.SemaphoreType.DMA(n)
    buf = lambda *n: pltpu.VMEM(n, BF)
    return pl.pallas_call(
        functools.partial(kernel, G, S, T, R, SL, NC),
        out_shape=jax.ShapeDtypeStruct((R, D), BF),
        in_specs=[vmem] * 8 + [hbm] * 3,
        out_specs=vmem,
        scratch_shapes=[
            buf(D, 2 * F), buf(F, D), buf(NC, T, GD, DC), buf(RIM, GD), buf(T, R, GD),
            buf(T, R, GD),
            buf(NC, S, SL, DC), buf(S, NC, T, SL, DC), buf(S, NC, T, SL, DC),
            buf(S, H, NC, SL, DC), buf(S, H, NC, SL, DC), buf(S, NC, SL, DC), buf(NC, S, SL, DC),
            pltpu.VMEM((T * SL, 2 * F), F32), buf(T * SL, F), buf(R, D), buf(R, D),
            pltpu.VMEM((S, 1, 128), F32), pltpu.VMEM((S, T, 1, 128), F32),
            dma(3), dma(H, NC), dma(H, NC), dma(H, G, NC), dma(H, G, NC), dma(H, NC), dma(H, NC),
            dma(1), dma(1), dma(T), dma(T),
            dma(S, NC), dma(S, NC), dma(S, H, NC), dma(S, H, NC), dma(S, H, NC), dma(S, H, NC),
            dma(S, H, NC), dma(S, H, NC), dma(S, H, NC), dma(S, H, NC), dma(S, NC), dma(S, NC),
            dma(S, T), dma(S, T),
        ],
        compiler_params=pltpu.CompilerParams(
            collective_id=0, has_side_effects=True, vmem_limit_bytes=63 * 1024 * 1024
        ),
    )(
        resid, pool_input, group_map, pool_scale.reshape(1, -1), out_proj,
        norm_gain, routes.T, route_weight.T,
        expert_gate[0], expert_up[0], expert_down[0],
    )


def solution(mesh):
    return jax.shard_map(
        local,
        mesh=mesh,
        in_specs=(
            P(("grp", "sp", "tp"), None),
            P(("grp", "sp"), "tp"),
            P("tp", None, None),
            P("tp"),
            P("tp", None),
            P(),
            P(("grp", "sp", "tp"), None),
            P(("grp", "sp", "tp"), None),
            P("sp", None, "tp"),
            P("sp", None, "tp"),
            P("sp", "tp", None),
        ),
        out_specs=P(("grp", "sp", "tp"), None),
        check_vma=False,
    )
```

```python
import functools

import jax
import jax.numpy as jnp
from jax import lax
from jax.experimental import pallas as pl
from jax.experimental.pallas import tpu as pltpu
from jax.sharding import PartitionSpec as P

GROUPS = 4
norm_eps = 1e-06
BF = jnp.bfloat16
F32 = jnp.float32
MESH = pl.DeviceIdType.MESH
RIM = 2**GROUPS
ORDER = ((0, 1, 2, 3), (1, 3, 0, 2), (2, 0, 3, 1), (3, 2, 1, 0))
SENDS = ((0, 2, 1, 3), (1, 3, 0, 2), (2, 0, 3, 1), (3, 1, 2, 0))


def nearest(s, j, S):
    low = jnp.minimum(s, S - 1 - s)
    half = (j + 1) // 2
    both = half * (2 * lax.rem(j, 2) - 1)
    rest = (j - low) * (1 - 2 * ((2 * s) // S))
    return s + jnp.where(j <= 2 * low, both * (1 - 2 * ((2 * s) // S)), rest)


def look_up(table, s, j):
    value = 0
    for a, row in enumerate(table):
        for b, entry in enumerate(row):
            value = value + jnp.where((s == a) & (j == b), entry, 0)
    return value


def visit(s, j, S):
    return look_up(ORDER, s, j) if S == 4 else nearest(s, lax.rem(S - j, S), S)


def sends(s, j, S):
    return look_up(SENDS, s, j) if S == 4 else nearest(s, S - j, S)


def kernel(
    G, S, T, R, SL, NC,
    resid, pool, gmap, scale, oproj, gain, routes_t, weight_t, wg, wu, wd,
    out,
    wgu_v, wd_v, opj, rim, piece, gout, stage, inbox, pbuf, rbuf, fbuf, fin, ret,
    acc, hid, mixed_v, rsend, rin,
    w_sem, ox_s, ox_r, oy_s, oy_r, on_s, on_r, rim_s, rim_r, pc_s, pc_r,
    z_s, z_r, f_s, f_r, n_s, n_r, pn_s, pn_r, pf_s, pf_r, rz_s, rz_r, rr_s, rr_r,
):
    g = lax.axis_index("grp")
    s = lax.axis_index("sp")
    t = lax.axis_index("tp")
    H = T // 2
    D = resid.shape[1]
    F = wd.shape[0]
    DC = D // NC
    GD = oproj.shape[0]
    GH = GD // G
    C = range(NC)
    near = t + 1 - 2 * lax.rem(t, 2)
    inner = (s != 0) & (s != S - 1)

    def cut(c):
        return slice(c * DC, (c + 1) * DC)

    def up(k):
        return lax.rem(t + 2 * k, T)

    def down(base, k):
        return lax.rem(base - 2 * k + 2 * T, T)

    def remote(src, dst, ss, rs, sp=None, tp=None, grp=None):
        return pltpu.make_async_remote_copy(
            src_ref=src, dst_ref=dst, send_sem=ss, recv_sem=rs,
            device_id={
                "grp": g if grp is None else grp,
                "sp": s if sp is None else sp,
                "tp": t if tp is None else tp,
            },
            device_id_type=MESH,
        )

    loads = [
        pltpu.make_async_copy(wg, wgu_v.at[:, pl.ds(0, F)], w_sem.at[0]),
        pltpu.make_async_copy(wu, wgu_v.at[:, pl.ds(F, F)], w_sem.at[1]),
        pltpu.make_async_copy(wd, wd_v, w_sem.at[2]),
    ]
    for load in loads:
        load.start()

    barrier = pltpu.get_barrier_semaphore()

    @pl.loop(1, S * T)
    def _(j):
        peer = lax.rem(s * T + t + j, S * T)
        pl.semaphore_signal(
            barrier, inc=1, device_id={"grp": g, "sp": peer // T, "tp": lax.rem(peer, T)},
            device_id_type=MESH,
        )

    for j in range(1, G):
        pl.semaphore_signal(
            barrier, inc=1, device_id={"grp": lax.rem(g + j, G), "sp": s, "tp": t},
            device_id_type=MESH,
        )
    pl.semaphore_wait(barrier, S * T - 1 + G - 1)

    seq = pool.shape[0]
    rim_copy = remote(
        pool.at[pl.ds(seq - RIM, RIM)], rim, rim_s.at[0], rim_r.at[0], sp=lax.rem(s + 1, S)
    )
    rim_copy.start()

    def own_rows(h):
        return pl.ds(pl.multiple_of(h * GH, GH), GH)

    def o_far(k, c):
        return remote(
            oproj.at[own_rows(g), cut(c)], opj.at[c, t, own_rows(g)],
            ox_s.at[k - 1], ox_r.at[k - 1, c], tp=up(k),
        )

    def o_part(k, j, c):
        part = opj.at[c, down(t, k), own_rows(g)]
        return remote(
            part, part, oy_s.at[k - 1, j - 1], oy_r.at[k - 1, j - 1, c], grp=lax.rem(g + j, G)
        )

    def o_near(k, c):
        block = opj.at[c, down(t, k)]
        return remote(
            oproj.at[:, cut(c)] if k == 0 else block, block, on_s.at[0], on_r.at[c], tp=near
        )

    def o_spread(c):
        for k in range(1, H):
            o_far(k, c).wait_recv()
            for j in range(1, G):
                o_part(k, j, c).start()

    def o_pass(c):
        for k in range(1, H):
            for j in range(1, G):
                o_part(k, j, c).wait_recv()
            o_near(k, c).start()

    for c in range(NC - 1):
        for k in range(1, H):
            o_far(k, c).start()
    for c in C:
        o_near(0, c).start()

    E = S
    EP = max(8, E)
    e_row = lax.broadcasted_iota(jnp.int32, (EP, R), 0)
    hot_row = [e_row == routes_t[k : k + 1, :] for k in range(2)]
    both_row = jnp.where(hot_row[0] | hot_row[1], 1.0, 0.0).astype(BF)
    before = lax.broadcasted_iota(jnp.int32, (R, R), 0) < lax.broadcasted_iota(
        jnp.int32, (R, R), 1
    )
    rank_row = jnp.dot(both_row, jnp.where(before, 1.0, 0.0).astype(BF), preferred_element_type=F32)
    slot_row = rank_row + (e_row * SL).astype(F32)
    tgt_row = [jnp.sum(jnp.where(h, slot_row, 0.0), axis=0, keepdims=True) for h in hot_row]

    eye = lax.broadcasted_iota(jnp.int32, (R, R), 0) == lax.broadcasted_iota(
        jnp.int32, (R, R), 1
    )

    def column(row):
        return jnp.sum(jnp.where(eye, row, 0.0), axis=1, keepdims=True)

    tgt_col = [column(row) for row in tgt_row]
    weight_col = [column(weight_t[k : k + 1, :]) for k in range(2)]

    rim_copy.wait_recv()
    values = pool[...].astype(F32)
    rim_v = jnp.where(s > 0, rim[...].astype(F32), 0.0)
    run = jnp.concatenate([rim_v, values], axis=0)
    window_sum = None
    for n in range(GROUPS):
        run = run + pltpu.roll(run, 2**n, 0)
        part = run[RIM:]
        window_sum = part if n == 0 else jnp.where(t >= n, part, window_sum)
    window = jnp.int32(2)
    for n in range(1, GROUPS):
        window = jnp.where(t >= n, jnp.int32(2 ** (n + 1)), window)
    position = s * seq + 1 + lax.broadcasted_iota(jnp.int32, (seq, GD), 0)
    divisor = jnp.minimum(position, window).astype(F32)
    pooled = (window_sum / divisor - values).astype(BF)
    product = jnp.dot(pooled, gmap[0], preferred_element_type=F32)
    piece[...] = (product * scale[...].astype(F32)).astype(BF).reshape(T, R, GD)

    def piece_copy(j):
        q = lax.rem(t + j, T)
        return remote(piece.at[q], gout.at[t], pc_s.at[0], pc_r.at[0], tp=q)

    for j in range(1, T):
        piece_copy(j).start()
    for k in range(1, H):
        o_far(k, NC - 1).start()
    gout[t] = piece[t]
    for c in C:
        opj[c, t] = oproj[:, cut(c)]

    slots = S * SL
    slot_iota = lax.broadcasted_iota(jnp.int32, (slots, R), 0).astype(F32)
    place = jnp.where((tgt_row[0] == slot_iota) | (tgt_row[1] == slot_iota), 1.0, 0.0).astype(BF)

    def z_copy(e, c):
        return remote(stage.at[c, e], inbox.at[s, c, t], z_s.at[0], z_r.at[s, c], sp=e)

    def z_arrival(i, c):
        return remote(stage.at[c, i], inbox.at[i, c, t], z_s.at[0], z_r.at[i, c], sp=i)

    def far_copy(i, k, c):
        block = inbox.at[i, c, t]
        return remote(block, block, f_s.at[k - 1], f_r.at[i, k - 1, c], tp=up(k))

    def near_copy(i, k, c):
        block = inbox.at[i, c, down(t, k)]
        return remote(block, block, n_s.at[0], n_r.at[i], tp=near)

    def r_copy(e, q, n):
        return remote(rsend.at[e], rin.at[s, t], rr_s.at[n], rr_r.at[s], sp=e, tp=q)

    def whole(ref, ss, rs):
        return remote(ref, ref, ss, rs, tp=near)

    def p_near(i, k, c):
        return remote(
            pbuf.at[i, c, down(near, k)], rbuf.at[i, c, k], pn_s.at[0], pn_r.at[i, c], tp=near
        )

    def p_far(i, k, c):
        q = down(t, k)
        return remote(
            pbuf.at[i, c, q], fbuf.at[i, k - 1, c], pf_s.at[k - 1], pf_r.at[i, k - 1, c], tp=q
        )

    def back(i, c):
        return remote(fin.at[i, c], ret.at[c, s], rz_s.at[0], rz_r.at[c], sp=i)

    def push(i, c):
        for k in range(1, H):
            far_copy(i, k, c).start()
        near_copy(i, 0, c).start()

    def fwd(p, c):
        i = visit(s, p, S)
        z_arrival(i, c).wait_recv()
        push(i, c)

    def relay(p, c):
        i = visit(s, p, S)
        for k in range(1, H):
            far_copy(i, k, c).wait_recv()
            near_copy(i, k, c).start()

    def ready(p):
        i = visit(s, p, S)
        whole(rbuf.at[i], n_s.at[0], n_r.at[i]).wait_recv()

        @pl.when(i != s)
        def _():
            whole(rin.at[i], rr_s.at[0], rr_r.at[i]).wait_recv()

        @pl.when(i == s)
        def _():
            whole(rin.at[i, pl.ds(0, T - 1)], rr_s.at[0], rr_r.at[i]).wait_recv()

    NT = 256 if (2 * F) % 256 == 0 else 128
    DT = 512
    GN = 2 * F // NT

    def hidden(p, lo, hi):
        i = visit(s, p, S)

        def one(n):
            cols = pl.ds(pl.multiple_of(n * NT, NT), NT)
            total = None
            for c in C:
                x = inbox[i, c].reshape(T * SL, DC)
                y = jnp.dot(x, wgu_v[cut(c), cols], preferred_element_type=F32)
                total = y if total is None else total + y
            acc[:, cols] = total

        for n in range(lo, hi):
            one(n)

    def gated(p):
        i = visit(s, p, S)
        spot = lax.broadcasted_iota(jnp.int32, (SL, 128), 0) == lax.broadcasted_iota(
            jnp.int32, (SL, 128), 1
        )
        for q in range(T):
            rows = slice(q * SL, (q + 1) * SL)
            r = jnp.sum(jnp.where(spot, rin[i, q], 0.0), axis=1, keepdims=True)
            gate = acc[rows, :F] * r
            hid[rows] = (gate / (1.0 + jnp.exp(-gate)) * (acc[rows, F:] * r)).astype(BF)

    def lower(p, c):
        i = visit(s, p, S)

        for n in range(DC // DT):
            y = jnp.dot(
                hid[...], wd_v[:, c * DC + n * DT : c * DC + (n + 1) * DT],
                preferred_element_type=F32,
            )
            pbuf[i, c, :, :, n * DT : (n + 1) * DT] = y.astype(BF).reshape(T, SL, DT)

        for k in range(H):
            p_near(i, k, c).start()

    def pair(p, c):
        i = visit(s, p, S)
        whole(rbuf.at[i, c], pn_s.at[0], pn_r.at[i, c]).wait_recv()
        for k in range(1, H):
            q = down(t, k)
            pbuf[i, c, q] = (pbuf[i, c, q].astype(F32) + rbuf[i, c, k].astype(F32)).astype(BF)
            p_far(i, k, c).start()

    def finish(p, c):
        i = visit(s, p, S)
        value = pbuf[i, c, t].astype(F32) + rbuf[i, c, 0].astype(F32)
        for k in range(1, H):
            p_far(i, k, c).wait_recv()
            value = value + fbuf[i, k - 1, c].astype(F32)
        return i, value.astype(BF)

    def send_back(p, c):
        i, value = finish(p, c)
        fin[i, c] = value
        back(i, c).start()

    def only(where, act, p, *c):
        @pl.when(where)
        def _():
            for n in c:
                act(p, n)

    def mix_part(c, wide, square):
        whole(opj.at[c, pl.ds(0, H)], on_s.at[0], on_r.at[c]).wait_recv()
        total = jnp.dot(wide, opj[c].reshape(T * GD, DC), preferred_element_type=F32)
        mixed = (resid[:, cut(c)].astype(F32) + total).astype(BF)
        mixed_v[:, cut(c)] = mixed
        residual = mixed.astype(F32)
        cast = (residual * gain[cut(c)].astype(F32).reshape(1, DC)).astype(BF)
        stage[c] = jnp.dot(place, cast, preferred_element_type=F32).astype(BF).reshape(S, SL, DC)
        inbox[s, c, t] = stage[c, s]

        z_copy(sends(s, 1, S), c).start()

        @pl.when(inner)
        def _():
            z_copy(sends(s, 2, S), c).start()

        push(s, c)
        return square + jnp.sum(residual * residual, axis=1, keepdims=True)

    square = jnp.zeros((R, 1), F32)
    o_spread(0)
    o_spread(1)
    for c in range(2, NC):
        o_pass(c - 2)
        o_spread(c)
    whole(gout.at[pl.ds(0, T - 1)], pc_s.at[0], pc_r.at[0]).wait_recv()
    wide = jnp.concatenate([gout[q] for q in range(T)], axis=1)
    for c in C:
        square = mix_part(c, wide, square)
        if c + 2 < NC:
            o_pass(c + NC - 2)
    unit = lax.rsqrt(square * (1.0 / D) + norm_eps)

    @pl.loop(0, S)
    def _(e):
        lane = (lax.broadcasted_iota(jnp.int32, (R, 128), 1) + e * SL).astype(F32)
        inside = lax.broadcasted_iota(jnp.int32, (R, 128), 1) < SL
        mine = ((tgt_col[0] == lane) | (tgt_col[1] == lane)) & inside
        rsend[e] = jnp.sum(jnp.where(mine, unit, 0.0), axis=0, keepdims=True)

    rin[s, t] = rsend[s]

    @pl.loop(1, T)
    def _(j):
        r_copy(s, lax.rem(t + j, T), 0).start()

    @pl.loop(0, (S - 1) * T)
    def _(j):
        r_copy(lax.rem(s + 1 + j // T, S), lax.rem(j, T), 1).start()

    @pl.loop(jnp.where(inner, 3, 2), S)
    def _(j):
        for c in C:
            z_copy(sends(s, j, S), c).start()

    for load in loads:
        load.wait()

    if S == 4:
        edge = (s == 0) | (s == S - 1)
        relay(0, 0)
        fwd(1, 0)
        relay(0, 1)
        fwd(1, 1)
        relay(0, 2)
        fwd(1, 2)
        relay(0, 3)
        ready(0)
        hidden(0, 0, 3)
        fwd(1, 3)
        relay(1, 0)
        hidden(0, 3, 5)
        hidden(0, 5, 7)
        relay(1, 1)
        fwd(2, 0)
        gated(0)
        lower(0, 0)
        relay(1, 2)
        lower(0, 1)
        fwd(2, 1)
        lower(0, 2)
        lower(0, 3)
        fwd(2, 2)
        relay(1, 3)
        ready(1)
        hidden(1, 0, 3)
        fwd(2, 3)
        only(inner, pair, 0, 0)
        relay(2, 0)
        hidden(1, 3, 5)
        relay(2, 1)
        hidden(1, 5, 7)
        only(edge, fwd, 3, 0)
        gated(1)
        relay(2, 2)
        lower(1, 0)
        only(edge, fwd, 3, 1)
        lower(1, 1)
        lower(1, 2)
        only(inner, pair, 1, 0)
        relay(2, 3)
        only(edge, fwd, 3, 2)
        lower(1, 3)
        only(inner, pair, 1, 1)
        only(edge, fwd, 3, 3)
        only(edge, pair, 1, 0)
        ready(2)
        only(inner, pair, 1, 2)
        hidden(2, 0, 3)
        only(inner, pair, 1, 3)
        only(inner, fwd, 3, 0)
        only(edge, relay, 3, 0)
        hidden(2, 3, 5)
        only(edge, relay, 3, 1)
        only(inner, fwd, 3, 1)
        only(inner, send_back, 1, 0)
        hidden(2, 5, 7)
        only(inner, fwd, 3, 2)
        gated(2)
        only(edge, relay, 3, 2)
        only(inner, send_back, 1, 1)
        lower(2, 0)
        only(inner, fwd, 3, 3)
        lower(2, 1)
        only(edge, pair, 2, 0)
        only(inner, send_back, 1, 2)
        lower(2, 2)
        only(edge, pair, 2, 1)
        only(edge, relay, 3, 3)
        lower(2, 3)
        only(inner, send_back, 1, 3)
        only(edge, pair, 2, 2, 3)
        only(edge, pair, 1, 1)
        only(inner, pair, 2, 0, 1, 2, 3)
        only(inner, pair, 0, 1)
        only(inner, relay, 3, 0, 1, 2, 3)
        ready(3)
        hidden(3, 0, 3)
        only(edge, send_back, 1, 0)
        only(edge, send_back, 2, 0)
        hidden(3, 3, 5)
        only(edge, send_back, 2, 1)
        only(inner, send_back, 2, 0)
        hidden(3, 5, 7)
        gated(3)
        only(edge, send_back, 2, 2)
        only(inner, send_back, 2, 1)
        lower(3, 0)
        lower(3, 1)
        lower(3, 2)
        pair(3, 0)
        pair(3, 1)
        only(inner, send_back, 2, 2)
        lower(3, 3)
        only(edge, send_back, 2, 3)
        pair(3, 2)
        pair(3, 3)
        only(edge, pair, 1, 2, 3)
        only(edge, pair, 0, 0, 1)
        pair(0, 2)
        pair(0, 3)
        only(inner, send_back, 2, 3)
        only(edge, send_back, 1, 1)
        send_back(3, 0)
        send_back(3, 1)
        send_back(3, 2)
        send_back(3, 3)
        only(edge, send_back, 1, 2, 3)
    else:
        @pl.loop(0, S + 1)
        def _(j):
            @pl.when(j < S)
            def _():
                for c in C:
                    relay(j, c)

            @pl.when(j + 1 < S)
            def _():
                for c in C:
                    fwd(j + 1, c)

            @pl.when(j > 1)
            def _():
                for c in C:
                    pair(j - 1, c)

            @pl.when(j < S)
            def _():
                ready(j)
                hidden(j, 0, GN)
                gated(j)
                for c in C:
                    lower(j, c)

            @pl.when(j > 1)
            def _():
                for c in C:
                    send_back(j - 1, c)

        for c in C:
            pair(0, c)

    lanes = lax.broadcasted_iota(jnp.int32, (R, slots), 1).astype(F32)
    pick = [jnp.where(tgt_col[k] == lanes, 1.0, 0.0).astype(BF) for k in range(2)]

    for c in C:
        _, value = finish(0, c)
        ret[c, s] = value
        whole(ret.at[c, pl.ds(0, S - 1)], rz_s.at[0], rz_r.at[c]).wait_recv()

        flat = ret[c].reshape(slots, DC)
        total = mixed_v[:, cut(c)].astype(F32)
        picked = [
            weight_col[k] * jnp.dot(pick[k], flat, preferred_element_type=F32) for k in range(2)
        ]
        out[:, cut(c)] = (total + (picked[0] + picked[1])).astype(BF)

    rim_copy.wait_send()
    half = opj.at[:, 0, pl.ds(0, GH)]
    for k in range(1, H):
        whole(half, ox_s.at[k - 1], ox_r.at[0, 0]).wait_send()
        for j in range(1, G):
            whole(half, oy_s.at[k - 1, j - 1], oy_r.at[0, 0, 0]).wait_send()
        whole(fin, f_s.at[k - 1], f_r.at[0, 0, 0]).wait_send()
        whole(fin, pf_s.at[k - 1], pf_r.at[0, 0, 0]).wait_send()
    whole(opj.at[:, pl.ds(0, H)], on_s.at[0], on_r.at[0]).wait_send()
    whole(piece.at[pl.ds(0, T - 1)], pc_s.at[0], pc_r.at[0]).wait_send()
    whole(rbuf, n_s.at[0], n_r.at[0]).wait_send()
    whole(rbuf, pn_s.at[0], pn_r.at[0, 0]).wait_send()
    others = fin.at[pl.ds(0, S - 1)]
    whole(others, z_s.at[0], z_r.at[0, 0]).wait_send()
    whole(others, rz_s.at[0], rz_r.at[0]).wait_send()
    whole(rin.at[0, pl.ds(0, T - 1)], rr_s.at[0], rr_r.at[0]).wait_send()
    whole(rin.at[pl.ds(0, S - 1)], rr_s.at[1], rr_r.at[0]).wait_send()


def local(
    resid, pool_input, group_map, pool_scale, out_proj, norm_gain, routes, route_weight,
    expert_gate, expert_up, expert_down,
):
    G, S, T = lax.axis_size("grp"), lax.axis_size("sp"), lax.axis_size("tp")
    R, D = resid.shape
    H = T // 2
    top = routes.shape[1]
    experts = S * expert_gate.shape[0]
    room = max(2, 5 * R * top // (4 * experts))
    SL = -(-room // 16) * 16
    F = expert_down.shape[1]
    GD = group_map.shape[1]
    NC = 4
    DC = D // NC
    vmem, hbm = pl.BlockSpec(memory_space=pltpu.VMEM), pl.BlockSpec(memory_space=pl.ANY)
    dma = lambda *n: pltpu.SemaphoreType.DMA(n)
    buf = lambda *n: pltpu.VMEM(n, BF)
    return pl.pallas_call(
        functools.partial(kernel, G, S, T, R, SL, NC),
        out_shape=jax.ShapeDtypeStruct((R, D), BF),
        in_specs=[vmem] * 8 + [hbm] * 3,
        out_specs=vmem,
        scratch_shapes=[
            buf(D, 2 * F), buf(F, D), buf(NC, T, GD, DC), buf(RIM, GD), buf(T, R, GD),
            buf(T, R, GD),
            buf(NC, S, SL, DC), buf(S, NC, T, SL, DC), buf(S, NC, T, SL, DC),
            buf(S, NC, H, SL, DC), buf(S, H - 1, NC, SL, DC), buf(S, NC, SL, DC),
            buf(NC, S, SL, DC),
            pltpu.VMEM((T * SL, 2 * F), F32), buf(T * SL, F), buf(R, D),
            pltpu.VMEM((S, 1, 128), F32), pltpu.VMEM((S, T, 1, 128), F32),
            dma(3), dma(H - 1), dma(H - 1, NC), dma(H - 1, G - 1), dma(H - 1, G - 1, NC),
            dma(1), dma(NC), dma(1), dma(1), dma(1), dma(1),
            dma(1), dma(S, NC), dma(H - 1), dma(S, H - 1, NC), dma(1), dma(S),
            dma(1), dma(S, NC), dma(H - 1), dma(S, H - 1, NC), dma(1), dma(NC), dma(2), dma(S),
        ],
        compiler_params=pltpu.CompilerParams(
            collective_id=0, has_side_effects=True, vmem_limit_bytes=63 * 1024 * 1024
        ),
    )(
        resid, pool_input, group_map, pool_scale.reshape(1, -1), out_proj,
        norm_gain, routes.T, route_weight.T,
        expert_gate[0], expert_up[0], expert_down[0],
    )


def solution(mesh):
    return jax.shard_map(
        local,
        mesh=mesh,
        in_specs=(
            P(("grp", "sp", "tp"), None),
            P(("grp", "sp"), "tp"),
            P("tp", None, None),
            P("tp"),
            P("tp", None),
            P(),
            P(("grp", "sp", "tp"), None),
            P(("grp", "sp", "tp"), None),
            P("sp", None, "tp"),
            P("sp", None, "tp"),
            P("sp", "tp", None),
        ),
        out_specs=P(("grp", "sp", "tp"), None),
        check_vma=False,
    )
```

```python
import functools

import jax
import jax.numpy as jnp
from jax import lax
from jax.experimental import pallas as pl
from jax.experimental.pallas import tpu as pltpu
from jax.sharding import PartitionSpec as P

GROUPS = 4
norm_eps = 1e-06
BF = jnp.bfloat16
F32 = jnp.float32
MESH = pl.DeviceIdType.MESH
RIM = 2**GROUPS
ORDER = ((0, 1, 2, 3), (1, 3, 0, 2), (2, 0, 3, 1), (3, 2, 1, 0))
SENDS = ((0, 2, 1, 3), (1, 3, 0, 2), (2, 0, 3, 1), (3, 1, 2, 0))


def nearest(s, j, S):
    low = jnp.minimum(s, S - 1 - s)
    half = (j + 1) // 2
    both = half * (2 * lax.rem(j, 2) - 1)
    rest = (j - low) * (1 - 2 * ((2 * s) // S))
    return s + jnp.where(j <= 2 * low, both * (1 - 2 * ((2 * s) // S)), rest)


def look_up(table, s, j):
    value = 0
    for a, row in enumerate(table):
        for b, entry in enumerate(row):
            value = value + jnp.where((s == a) & (j == b), entry, 0)
    return value


def visit(s, j, S):
    return look_up(ORDER, s, j) if S == 4 else nearest(s, lax.rem(S - j, S), S)


def sends(s, j, S):
    return look_up(SENDS, s, j) if S == 4 else nearest(s, S - j, S)


def kernel(
    G, S, T, R, SL, NC,
    resid_h, pool_h, gmap_h, scale_h, oproj_h, gain_h, routes_h, weight_h, wg, wu, wd,
    out_h,
    oproj, pool, resid, gmap, scale, gain, routes_t, weight_t, out,
    wgu_v, wd_v, opj, rim, piece, gout, stage, inbox, pbuf, rbuf, fbuf, fin, ret,
    acc, hid, mixed_v, rsend, rin,
    w_sem, i_sem, ox_s, ox_r, oy_s, oy_r, on_s, on_r, rim_s, rim_r, pc_s, pc_r,
    z_s, z_r, f_s, f_r, n_s, n_r, pn_s, pn_r, pf_s, pf_r, rz_s, rz_r, rr_s, rr_r,
):
    g = lax.axis_index("grp")
    s = lax.axis_index("sp")
    t = lax.axis_index("tp")
    H = T // 2
    D = resid.shape[1]
    F = wd.shape[0]
    DC = D // NC
    GD = oproj.shape[0]
    GH = GD // G
    C = range(NC)
    near = t + 1 - 2 * lax.rem(t, 2)
    inner = (s != 0) & (s != S - 1)

    def cut(c):
        return slice(c * DC, (c + 1) * DC)

    def up(k):
        return lax.rem(t + 2 * k, T)

    def down(base, k):
        return lax.rem(base - 2 * k + 2 * T, T)

    def remote(src, dst, ss, rs, sp=None, tp=None, grp=None):
        return pltpu.make_async_remote_copy(
            src_ref=src, dst_ref=dst, send_sem=ss, recv_sem=rs,
            device_id={
                "grp": g if grp is None else grp,
                "sp": s if sp is None else sp,
                "tp": t if tp is None else tp,
            },
            device_id_type=MESH,
        )

    barrier = pltpu.get_barrier_semaphore()

    @pl.loop(1, S * T)
    def _(j):
        peer = lax.rem(s * T + t + j, S * T)
        pl.semaphore_signal(
            barrier, inc=1, device_id={"grp": g, "sp": peer // T, "tp": lax.rem(peer, T)},
            device_id_type=MESH,
        )

    for j in range(1, G):
        pl.semaphore_signal(
            barrier, inc=1, device_id={"grp": lax.rem(g + j, G), "sp": s, "tp": t},
            device_id_type=MESH,
        )
    pairs = (
        (oproj_h, oproj), (pool_h, pool), (resid_h, resid), (gmap_h, gmap), (scale_h, scale),
        (gain_h, gain), (routes_h, routes_t), (weight_h, weight_t),
    )
    takes = [pltpu.make_async_copy(a, b, i_sem.at[n]) for n, (a, b) in enumerate(pairs)]
    for take in takes:
        take.start()
    loads = [
        pltpu.make_async_copy(wg, wgu_v.at[:, pl.ds(0, F)], w_sem.at[0]),
        pltpu.make_async_copy(wu, wgu_v.at[:, pl.ds(F, F)], w_sem.at[1]),
        pltpu.make_async_copy(wd, wd_v, w_sem.at[2]),
    ]
    for load in loads:
        load.start()

    for take in takes:
        take.wait()
    pl.semaphore_wait(barrier, S * T - 1 + G - 1)

    seq = pool.shape[0]
    rim_copy = remote(
        pool.at[pl.ds(seq - RIM, RIM)], rim, rim_s.at[0], rim_r.at[0], sp=lax.rem(s + 1, S)
    )
    rim_copy.start()

    def own_rows(h):
        return pl.ds(pl.multiple_of(h * GH, GH), GH)

    def o_far(k, c):
        return remote(
            oproj.at[own_rows(g), cut(c)], opj.at[c, t, own_rows(g)],
            ox_s.at[k - 1], ox_r.at[k - 1, c], tp=up(k),
        )

    def o_part(k, j, c):
        part = opj.at[c, down(t, k), own_rows(g)]
        return remote(
            part, part, oy_s.at[k - 1, j - 1], oy_r.at[k - 1, j - 1, c], grp=lax.rem(g + j, G)
        )

    def o_near(k, c):
        block = opj.at[c, down(t, k)]
        return remote(
            oproj.at[:, cut(c)] if k == 0 else block, block, on_s.at[0], on_r.at[c], tp=near
        )

    def o_spread(c):
        for k in range(1, H):
            o_far(k, c).wait_recv()
            for j in range(1, G):
                o_part(k, j, c).start()

    def o_pass(c):
        for k in range(1, H):
            for j in range(1, G):
                o_part(k, j, c).wait_recv()
            o_near(k, c).start()

    for c in range(NC - 1):
        for k in range(1, H):
            o_far(k, c).start()
    for c in C:
        o_near(0, c).start()

    E = S
    EP = max(8, E)
    e_row = lax.broadcasted_iota(jnp.int32, (EP, R), 0)
    hot_row = [e_row == routes_t[k : k + 1, :] for k in range(2)]
    both_row = jnp.where(hot_row[0] | hot_row[1], 1.0, 0.0).astype(BF)
    before = lax.broadcasted_iota(jnp.int32, (R, R), 0) < lax.broadcasted_iota(
        jnp.int32, (R, R), 1
    )
    rank_row = jnp.dot(both_row, jnp.where(before, 1.0, 0.0).astype(BF), preferred_element_type=F32)
    slot_row = rank_row + (e_row * SL).astype(F32)
    tgt_row = [jnp.sum(jnp.where(h, slot_row, 0.0), axis=0, keepdims=True) for h in hot_row]

    eye = lax.broadcasted_iota(jnp.int32, (R, R), 0) == lax.broadcasted_iota(
        jnp.int32, (R, R), 1
    )

    def column(row):
        return jnp.sum(jnp.where(eye, row, 0.0), axis=1, keepdims=True)

    tgt_col = [column(row) for row in tgt_row]
    weight_col = [column(weight_t[k : k + 1, :]) for k in range(2)]

    rim_copy.wait_recv()
    values = pool[...].astype(F32)
    rim_v = jnp.where(s > 0, rim[...].astype(F32), 0.0)
    run = jnp.concatenate([rim_v, values], axis=0)
    window_sum = None
    for n in range(GROUPS):
        run = run + pltpu.roll(run, 2**n, 0)
        part = run[RIM:]
        window_sum = part if n == 0 else jnp.where(t >= n, part, window_sum)
    window = jnp.int32(2)
    for n in range(1, GROUPS):
        window = jnp.where(t >= n, jnp.int32(2 ** (n + 1)), window)
    position = s * seq + 1 + lax.broadcasted_iota(jnp.int32, (seq, GD), 0)
    divisor = jnp.minimum(position, window).astype(F32)
    pooled = (window_sum / divisor - values).astype(BF)
    product = jnp.dot(pooled, gmap[0], preferred_element_type=F32)
    piece[...] = (product * scale[...].astype(F32)).astype(BF).reshape(T, R, GD)

    def piece_copy(j):
        q = lax.rem(t + j, T)
        return remote(piece.at[q], gout.at[t], pc_s.at[0], pc_r.at[0], tp=q)

    for j in range(1, T):
        piece_copy(j).start()
    for k in range(1, H):
        o_far(k, NC - 1).start()
    gout[t] = piece[t]
    for c in C:
        opj[c, t] = oproj[:, cut(c)]

    slots = S * SL
    slot_iota = lax.broadcasted_iota(jnp.int32, (slots, R), 0).astype(F32)
    place = jnp.where((tgt_row[0] == slot_iota) | (tgt_row[1] == slot_iota), 1.0, 0.0).astype(BF)

    def z_copy(e, c):
        return remote(stage.at[c, e], inbox.at[s, c, t], z_s.at[0], z_r.at[s, c], sp=e)

    def z_arrival(i, c):
        return remote(stage.at[c, i], inbox.at[i, c, t], z_s.at[0], z_r.at[i, c], sp=i)

    def far_copy(i, k, c):
        block = inbox.at[i, c, t]
        return remote(block, block, f_s.at[k - 1], f_r.at[i, k - 1, c], tp=up(k))

    def near_copy(i, k, c):
        block = inbox.at[i, c, down(t, k)]
        return remote(block, block, n_s.at[0], n_r.at[i], tp=near)

    def r_copy(e, q, n):
        return remote(rsend.at[e], rin.at[s, t], rr_s.at[n], rr_r.at[s], sp=e, tp=q)

    def whole(ref, ss, rs):
        return remote(ref, ref, ss, rs, tp=near)

    def p_near(i, k, c):
        return remote(
            pbuf.at[i, c, down(near, k)], rbuf.at[i, c, k], pn_s.at[0], pn_r.at[i, c], tp=near
        )

    def p_far(i, k, c):
        q = down(t, k)
        return remote(
            pbuf.at[i, c, q], fbuf.at[i, k - 1, c], pf_s.at[k - 1], pf_r.at[i, k - 1, c], tp=q
        )

    def back(i, c):
        return remote(fin.at[i, c], ret.at[c, s], rz_s.at[0], rz_r.at[c], sp=i)

    def push(i, c):
        for k in range(1, H):
            far_copy(i, k, c).start()
        near_copy(i, 0, c).start()

    def fwd(p, c):
        i = visit(s, p, S)
        z_arrival(i, c).wait_recv()
        push(i, c)

    def relay(p, c):
        i = visit(s, p, S)
        for k in range(1, H):
            far_copy(i, k, c).wait_recv()
            near_copy(i, k, c).start()

    def ready(p):
        i = visit(s, p, S)
        whole(rbuf.at[i], n_s.at[0], n_r.at[i]).wait_recv()

        @pl.when(i != s)
        def _():
            whole(rin.at[i], rr_s.at[0], rr_r.at[i]).wait_recv()

        @pl.when(i == s)
        def _():
            whole(rin.at[i, pl.ds(0, T - 1)], rr_s.at[0], rr_r.at[i]).wait_recv()

    NT = 256 if (2 * F) % 256 == 0 else 128
    DT = 512
    GN = 2 * F // NT

    def hidden(p, lo, hi):
        i = visit(s, p, S)

        def one(n):
            cols = pl.ds(pl.multiple_of(n * NT, NT), NT)
            total = None
            for c in C:
                x = inbox[i, c].reshape(T * SL, DC)
                y = jnp.dot(x, wgu_v[cut(c), cols], preferred_element_type=F32)
                total = y if total is None else total + y
            acc[:, cols] = total

        for n in range(lo, hi):
            one(n)

    def gated(p):
        i = visit(s, p, S)
        spot = lax.broadcasted_iota(jnp.int32, (SL, 128), 0) == lax.broadcasted_iota(
            jnp.int32, (SL, 128), 1
        )
        for q in range(T):
            rows = slice(q * SL, (q + 1) * SL)
            r = jnp.sum(jnp.where(spot, rin[i, q], 0.0), axis=1, keepdims=True)
            gate = acc[rows, :F] * r
            hid[rows] = (gate / (1.0 + jnp.exp(-gate)) * (acc[rows, F:] * r)).astype(BF)

    def lower(p, c):
        i = visit(s, p, S)

        for n in range(DC // DT):
            y = jnp.dot(
                hid[...], wd_v[:, c * DC + n * DT : c * DC + (n + 1) * DT],
                preferred_element_type=F32,
            )
            pbuf[i, c, :, :, n * DT : (n + 1) * DT] = y.astype(BF).reshape(T, SL, DT)

        for k in range(H):
            p_near(i, k, c).start()

    def pair(p, c):
        i = visit(s, p, S)
        whole(rbuf.at[i, c], pn_s.at[0], pn_r.at[i, c]).wait_recv()
        for k in range(1, H):
            q = down(t, k)
            pbuf[i, c, q] = (pbuf[i, c, q].astype(F32) + rbuf[i, c, k].astype(F32)).astype(BF)
            p_far(i, k, c).start()

    def finish(p, c):
        i = visit(s, p, S)
        value = pbuf[i, c, t].astype(F32) + rbuf[i, c, 0].astype(F32)
        for k in range(1, H):
            p_far(i, k, c).wait_recv()
            value = value + fbuf[i, k - 1, c].astype(F32)
        return i, value.astype(BF)

    def send_back(p, c):
        i, value = finish(p, c)
        fin[i, c] = value
        back(i, c).start()

    def only(where, act, p, *c):
        @pl.when(where)
        def _():
            for n in c:
                act(p, n)

    def mix_part(c, wide, square):
        whole(opj.at[c, pl.ds(0, H)], on_s.at[0], on_r.at[c]).wait_recv()
        total = jnp.dot(wide, opj[c].reshape(T * GD, DC), preferred_element_type=F32)
        mixed = (resid[:, cut(c)].astype(F32) + total).astype(BF)
        mixed_v[:, cut(c)] = mixed
        residual = mixed.astype(F32)
        cast = (residual * gain[cut(c)].astype(F32).reshape(1, DC)).astype(BF)
        stage[c] = jnp.dot(place, cast, preferred_element_type=F32).astype(BF).reshape(S, SL, DC)
        inbox[s, c, t] = stage[c, s]

        z_copy(sends(s, 1, S), c).start()

        @pl.when(inner)
        def _():
            z_copy(sends(s, 2, S), c).start()

        push(s, c)
        return square + jnp.sum(residual * residual, axis=1, keepdims=True)

    square = jnp.zeros((R, 1), F32)
    o_spread(0)
    o_spread(1)
    for c in range(2, NC):
        o_pass(c - 2)
        o_spread(c)
    whole(gout.at[pl.ds(0, T - 1)], pc_s.at[0], pc_r.at[0]).wait_recv()
    wide = jnp.concatenate([gout[q] for q in range(T)], axis=1)
    for c in C:
        square = mix_part(c, wide, square)
        if c + 2 < NC:
            o_pass(c + NC - 2)
    unit = lax.rsqrt(square * (1.0 / D) + norm_eps)

    @pl.loop(0, S)
    def _(e):
        lane = (lax.broadcasted_iota(jnp.int32, (R, 128), 1) + e * SL).astype(F32)
        inside = lax.broadcasted_iota(jnp.int32, (R, 128), 1) < SL
        mine = ((tgt_col[0] == lane) | (tgt_col[1] == lane)) & inside
        rsend[e] = jnp.sum(jnp.where(mine, unit, 0.0), axis=0, keepdims=True)

    rin[s, t] = rsend[s]

    @pl.loop(1, T)
    def _(j):
        r_copy(s, lax.rem(t + j, T), 0).start()

    @pl.loop(0, (S - 1) * T)
    def _(j):
        r_copy(lax.rem(s + 1 + j // T, S), lax.rem(j, T), 1).start()

    @pl.loop(jnp.where(inner, 3, 2), S)
    def _(j):
        for c in C:
            z_copy(sends(s, j, S), c).start()

    for load in loads:
        load.wait()

    if S == 4:
        edge = (s == 0) | (s == S - 1)
        relay(0, 0)
        fwd(1, 0)
        relay(0, 1)
        fwd(1, 1)
        relay(0, 2)
        fwd(1, 2)
        relay(0, 3)
        ready(0)
        hidden(0, 0, 3)
        fwd(1, 3)
        relay(1, 0)
        hidden(0, 3, 5)
        hidden(0, 5, 7)
        relay(1, 1)
        fwd(2, 0)
        gated(0)
        lower(0, 0)
        relay(1, 2)
        lower(0, 1)
        fwd(2, 1)
        lower(0, 2)
        lower(0, 3)
        fwd(2, 2)
        relay(1, 3)
        ready(1)
        hidden(1, 0, 3)
        fwd(2, 3)
        only(inner, pair, 0, 0)
        relay(2, 0)
        hidden(1, 3, 5)
        relay(2, 1)
        hidden(1, 5, 7)
        only(edge, fwd, 3, 0)
        gated(1)
        relay(2, 2)
        lower(1, 0)
        only(edge, fwd, 3, 1)
        lower(1, 1)
        lower(1, 2)
        only(inner, pair, 1, 0)
        relay(2, 3)
        only(edge, fwd, 3, 2)
        lower(1, 3)
        only(inner, pair, 1, 1)
        only(edge, fwd, 3, 3)
        only(edge, pair, 1, 0)
        ready(2)
        only(inner, pair, 1, 2)
        hidden(2, 0, 3)
        only(inner, pair, 1, 3)
        only(inner, fwd, 3, 0)
        only(edge, relay, 3, 0)
        hidden(2, 3, 5)
        only(edge, relay, 3, 1)
        only(inner, fwd, 3, 1)
        only(inner, send_back, 1, 0)
        hidden(2, 5, 7)
        only(inner, fwd, 3, 2)
        gated(2)
        only(edge, relay, 3, 2)
        only(inner, send_back, 1, 1)
        lower(2, 0)
        only(inner, fwd, 3, 3)
        lower(2, 1)
        only(edge, pair, 2, 0)
        only(inner, send_back, 1, 2)
        lower(2, 2)
        only(edge, pair, 2, 1)
        only(edge, relay, 3, 3)
        lower(2, 3)
        only(inner, send_back, 1, 3)
        only(edge, pair, 2, 2, 3)
        only(edge, pair, 1, 1)
        only(inner, pair, 2, 0, 1, 2, 3)
        only(inner, pair, 0, 1)
        only(inner, relay, 3, 0, 1, 2, 3)
        ready(3)
        hidden(3, 0, 3)
        only(edge, send_back, 1, 0)
        only(edge, send_back, 2, 0)
        hidden(3, 3, 5)
        only(edge, send_back, 2, 1)
        only(inner, send_back, 2, 0)
        hidden(3, 5, 7)
        gated(3)
        only(edge, send_back, 2, 2)
        only(inner, send_back, 2, 1)
        lower(3, 0)
        lower(3, 1)
        lower(3, 2)
        pair(3, 0)
        pair(3, 1)
        only(inner, send_back, 2, 2)
        lower(3, 3)
        only(edge, send_back, 2, 3)
        pair(3, 2)
        pair(3, 3)
        only(edge, pair, 1, 2, 3)
        only(edge, pair, 0, 0, 1)
        pair(0, 2)
        pair(0, 3)
        only(inner, send_back, 2, 3)
        only(edge, send_back, 1, 1)
        send_back(3, 0)
        send_back(3, 1)
        send_back(3, 2)
        send_back(3, 3)
        only(edge, send_back, 1, 2, 3)
    else:
        @pl.loop(0, S + 1)
        def _(j):
            @pl.when(j < S)
            def _():
                for c in C:
                    relay(j, c)

            @pl.when(j + 1 < S)
            def _():
                for c in C:
                    fwd(j + 1, c)

            @pl.when(j > 1)
            def _():
                for c in C:
                    pair(j - 1, c)

            @pl.when(j < S)
            def _():
                ready(j)
                hidden(j, 0, GN)
                gated(j)
                for c in C:
                    lower(j, c)

            @pl.when(j > 1)
            def _():
                for c in C:
                    send_back(j - 1, c)

        for c in C:
            pair(0, c)

    lanes = lax.broadcasted_iota(jnp.int32, (R, slots), 1).astype(F32)
    pick = [jnp.where(tgt_col[k] == lanes, 1.0, 0.0).astype(BF) for k in range(2)]

    for c in C:
        _, value = finish(0, c)
        ret[c, s] = value
        whole(ret.at[c, pl.ds(0, S - 1)], rz_s.at[0], rz_r.at[c]).wait_recv()

        flat = ret[c].reshape(slots, DC)
        total = mixed_v[:, cut(c)].astype(F32)
        picked = [
            weight_col[k] * jnp.dot(pick[k], flat, preferred_element_type=F32) for k in range(2)
        ]
        out[:, cut(c)] = (total + (picked[0] + picked[1])).astype(BF)
        pltpu.make_async_copy(out.at[:, cut(c)], out_h.at[:, cut(c)], w_sem.at[3]).start()

    rim_copy.wait_send()
    half = opj.at[:, 0, pl.ds(0, GH)]
    for k in range(1, H):
        whole(half, ox_s.at[k - 1], ox_r.at[0, 0]).wait_send()
        for j in range(1, G):
            whole(half, oy_s.at[k - 1, j - 1], oy_r.at[0, 0, 0]).wait_send()
        whole(fin, f_s.at[k - 1], f_r.at[0, 0, 0]).wait_send()
        whole(fin, pf_s.at[k - 1], pf_r.at[0, 0, 0]).wait_send()
    whole(opj.at[:, pl.ds(0, H)], on_s.at[0], on_r.at[0]).wait_send()
    whole(piece.at[pl.ds(0, T - 1)], pc_s.at[0], pc_r.at[0]).wait_send()
    whole(rbuf, n_s.at[0], n_r.at[0]).wait_send()
    whole(rbuf, pn_s.at[0], pn_r.at[0, 0]).wait_send()
    others = fin.at[pl.ds(0, S - 1)]
    whole(others, z_s.at[0], z_r.at[0, 0]).wait_send()
    whole(others, rz_s.at[0], rz_r.at[0]).wait_send()
    whole(rin.at[0, pl.ds(0, T - 1)], rr_s.at[0], rr_r.at[0]).wait_send()
    whole(rin.at[pl.ds(0, S - 1)], rr_s.at[1], rr_r.at[0]).wait_send()
    pltpu.make_async_copy(out, out_h, w_sem.at[3]).wait()


def local(
    resid, pool_input, group_map, pool_scale, out_proj, norm_gain, routes, route_weight,
    expert_gate, expert_up, expert_down,
):
    G, S, T = lax.axis_size("grp"), lax.axis_size("sp"), lax.axis_size("tp")
    R, D = resid.shape
    H = T // 2
    top = routes.shape[1]
    experts = S * expert_gate.shape[0]
    room = max(2, 5 * R * top // (4 * experts))
    SL = -(-room // 16) * 16
    F = expert_down.shape[1]
    GD = group_map.shape[1]
    NC = 4
    DC = D // NC
    hbm = pl.BlockSpec(memory_space=pl.ANY)
    dma = lambda *n: pltpu.SemaphoreType.DMA(n)
    buf = lambda *n: pltpu.VMEM(n, BF)
    return pl.pallas_call(
        functools.partial(kernel, G, S, T, R, SL, NC),
        out_shape=jax.ShapeDtypeStruct((R, D), BF),
        in_specs=[hbm] * 11,
        out_specs=hbm,
        scratch_shapes=[
            buf(GD, D), buf(pool_input.shape[0], GD), buf(R, D), buf(1, GD, GD), buf(1, GD), buf(D),
            pltpu.VMEM((top, R), jnp.int32), pltpu.VMEM((top, R), F32), buf(R, D),
            buf(D, 2 * F), buf(F, D), buf(NC, T, GD, DC), buf(RIM, GD), buf(T, R, GD),
            buf(T, R, GD),
            buf(NC, S, SL, DC), buf(S, NC, T, SL, DC), buf(S, NC, T, SL, DC),
            buf(S, NC, H, SL, DC), buf(S, H - 1, NC, SL, DC), buf(S, NC, SL, DC),
            buf(NC, S, SL, DC),
            pltpu.VMEM((T * SL, 2 * F), F32), buf(T * SL, F), buf(R, D),
            pltpu.VMEM((S, 1, 128), F32), pltpu.VMEM((S, T, 1, 128), F32),
            dma(4), dma(8), dma(H - 1), dma(H - 1, NC), dma(H - 1, G - 1), dma(H - 1, G - 1, NC),
            dma(1), dma(NC), dma(1), dma(1), dma(1), dma(1),
            dma(1), dma(S, NC), dma(H - 1), dma(S, H - 1, NC), dma(1), dma(S),
            dma(1), dma(S, NC), dma(H - 1), dma(S, H - 1, NC), dma(1), dma(NC), dma(2), dma(S),
        ],
        compiler_params=pltpu.CompilerParams(
            collective_id=0, has_side_effects=True, vmem_limit_bytes=63 * 1024 * 1024
        ),
    )(
        resid, pool_input, group_map, pool_scale.reshape(1, -1), out_proj,
        norm_gain, routes.T, route_weight.T,
        expert_gate[0], expert_up[0], expert_down[0],
    )


def solution(mesh):
    return jax.shard_map(
        local,
        mesh=mesh,
        in_specs=(
            P(("grp", "sp", "tp"), None),
            P(("grp", "sp"), "tp"),
            P("tp", None, None),
            P("tp"),
            P("tp", None),
            P(),
            P(("grp", "sp", "tp"), None),
            P(("grp", "sp", "tp"), None),
            P("sp", None, "tp"),
            P("sp", None, "tp"),
            P("sp", "tp", None),
        ),
        out_specs=P(("grp", "sp", "tp"), None),
        check_vma=False,
    )
```

```python
import functools

import jax
import jax.numpy as jnp
from jax import lax
from jax.experimental import pallas as pl
from jax.experimental.pallas import tpu as pltpu
from jax.sharding import PartitionSpec as P

GROUPS = 4
norm_eps = 1e-06
BF = jnp.bfloat16
F32 = jnp.float32
MESH = pl.DeviceIdType.MESH
RIM = 2**GROUPS
ORDER = ((0, 1, 2, 3), (1, 3, 0, 2), (2, 0, 3, 1), (3, 2, 1, 0))
SENDS = ((0, 2, 1, 3), (1, 3, 0, 2), (2, 0, 3, 1), (3, 1, 2, 0))


def nearest(s, j, S):
    low = jnp.minimum(s, S - 1 - s)
    half = (j + 1) // 2
    both = half * (2 * lax.rem(j, 2) - 1)
    rest = (j - low) * (1 - 2 * ((2 * s) // S))
    return s + jnp.where(j <= 2 * low, both * (1 - 2 * ((2 * s) // S)), rest)


def look_up(table, s, j):
    value = 0
    for a, row in enumerate(table):
        for b, entry in enumerate(row):
            value = value + jnp.where((s == a) & (j == b), entry, 0)
    return value


def visit(s, j, S):
    return look_up(ORDER, s, j) if S == 4 else nearest(s, lax.rem(S - j, S), S)


def sends(s, j, S):
    return look_up(SENDS, s, j) if S == 4 else nearest(s, S - j, S)


def kernel(
    G, S, T, R, SL, NC,
    resid_h, pool_h, gmap_h, scale_h, oproj_h, gain_h, routes_h, weight_h, wg, wu, wd,
    out_h,
    oproj, pool, resid, gmap, scale, gain, routes_t, weight_t, out,
    wgu_v, wd_v, opj, rim, piece, gout, stage, inbox, pbuf, rbuf, fbuf, fin, ret,
    acc, hid, mixed_v, rsend, rin,
    w_sem, i_sem, ox_s, ox_r, oy_s, oy_r, on_s, on_r, rim_s, rim_r, pc_s, pc_r,
    z_s, z_r, f_s, f_r, n_s, n_r, pn_s, pn_r, pf_s, pf_r, rz_s, rz_r, rr_s, rr_r,
):
    g = lax.axis_index("grp")
    s = lax.axis_index("sp")
    t = lax.axis_index("tp")
    H = T // 2
    D = resid.shape[1]
    F = wd.shape[0]
    DC = D // NC
    GD = oproj.shape[0]
    GH = GD // G
    C = range(NC)
    near = t + 1 - 2 * lax.rem(t, 2)
    inner = (s != 0) & (s != S - 1)

    def cut(c):
        return slice(c * DC, (c + 1) * DC)

    def up(k):
        return lax.rem(t + 2 * k, T)

    def down(base, k):
        return lax.rem(base - 2 * k + 2 * T, T)

    def remote(src, dst, ss, rs, sp=None, tp=None, grp=None):
        return pltpu.make_async_remote_copy(
            src_ref=src, dst_ref=dst, send_sem=ss, recv_sem=rs,
            device_id={
                "grp": g if grp is None else grp,
                "sp": s if sp is None else sp,
                "tp": t if tp is None else tp,
            },
            device_id_type=MESH,
        )

    barrier = pltpu.get_barrier_semaphore()

    @pl.loop(1, S)
    def _(j):
        pl.semaphore_signal(
            barrier, inc=1, device_id={"grp": g, "sp": lax.rem(s + j, S), "tp": t},
            device_id_type=MESH,
        )

    for j in range(1, T):
        pl.semaphore_signal(
            barrier, inc=1, device_id={"grp": g, "sp": s, "tp": lax.rem(t + j, T)},
            device_id_type=MESH,
        )

    for j in range(1, G):
        pl.semaphore_signal(
            barrier, inc=1, device_id={"grp": lax.rem(g + j, G), "sp": s, "tp": t},
            device_id_type=MESH,
        )
    pairs = (
        (oproj_h, oproj), (pool_h, pool), (resid_h, resid), (gmap_h, gmap), (scale_h, scale),
        (gain_h, gain), (routes_h, routes_t), (weight_h, weight_t),
    )
    takes = [pltpu.make_async_copy(a, b, i_sem.at[n]) for n, (a, b) in enumerate(pairs)]
    for take in takes:
        take.start()
    loads = [
        pltpu.make_async_copy(wg, wgu_v.at[:, pl.ds(0, F)], w_sem.at[0]),
        pltpu.make_async_copy(wu, wgu_v.at[:, pl.ds(F, F)], w_sem.at[1]),
        pltpu.make_async_copy(wd, wd_v, w_sem.at[2]),
    ]
    for load in loads:
        load.start()

    for take in takes:
        take.wait()
    pl.semaphore_wait(barrier, S - 1 + T - 1 + G - 1)

    seq = pool.shape[0]
    rim_copy = remote(
        pool.at[pl.ds(seq - RIM, RIM)], rim, rim_s.at[0], rim_r.at[0], sp=lax.rem(s + 1, S)
    )
    rim_copy.start()

    def own_rows(h):
        return pl.ds(pl.multiple_of(h * GH, GH), GH)

    def o_far(k, c):
        return remote(
            oproj.at[own_rows(g), cut(c)], opj.at[c, t, own_rows(g)],
            ox_s.at[k - 1], ox_r.at[k - 1, c], tp=up(k),
        )

    def o_part(k, j, c):
        part = opj.at[c, down(t, k), own_rows(g)]
        return remote(
            part, part, oy_s.at[k - 1, j - 1], oy_r.at[k - 1, j - 1, c], grp=lax.rem(g + j, G)
        )

    def o_near(k, c):
        block = opj.at[c, down(t, k)]
        return remote(
            oproj.at[:, cut(c)] if k == 0 else block, block, on_s.at[0], on_r.at[c], tp=near
        )

    def o_spread(c):
        for k in range(1, H):
            o_far(k, c).wait_recv()
            for j in range(1, G):
                o_part(k, j, c).start()

    def o_pass(c):
        for k in range(1, H):
            for j in range(1, G):
                o_part(k, j, c).wait_recv()
            o_near(k, c).start()

    for c in range(NC - 1):
        for k in range(1, H):
            o_far(k, c).start()
    for c in C:
        o_near(0, c).start()

    E = S
    EP = max(8, E)
    e_row = lax.broadcasted_iota(jnp.int32, (EP, R), 0)
    hot_row = [e_row == routes_t[k : k + 1, :] for k in range(2)]
    both_row = jnp.where(hot_row[0] | hot_row[1], 1.0, 0.0).astype(BF)
    before = lax.broadcasted_iota(jnp.int32, (R, R), 0) < lax.broadcasted_iota(
        jnp.int32, (R, R), 1
    )
    rank_row = jnp.dot(both_row, jnp.where(before, 1.0, 0.0).astype(BF), preferred_element_type=F32)
    slot_row = rank_row + (e_row * SL).astype(F32)
    tgt_row = [jnp.sum(jnp.where(h, slot_row, 0.0), axis=0, keepdims=True) for h in hot_row]

    eye = lax.broadcasted_iota(jnp.int32, (R, R), 0) == lax.broadcasted_iota(
        jnp.int32, (R, R), 1
    )

    def column(row):
        return jnp.sum(jnp.where(eye, row, 0.0), axis=1, keepdims=True)

    tgt_col = [column(row) for row in tgt_row]
    weight_col = [column(weight_t[k : k + 1, :]) for k in range(2)]

    rim_copy.wait_recv()
    values = pool[...].astype(F32)
    rim_v = jnp.where(s > 0, rim[...].astype(F32), 0.0)
    run = jnp.concatenate([rim_v, values], axis=0)
    window_sum = None
    for n in range(GROUPS):
        run = run + pltpu.roll(run, 2**n, 0)
        part = run[RIM:]
        window_sum = part if n == 0 else jnp.where(t >= n, part, window_sum)
    window = jnp.int32(2)
    for n in range(1, GROUPS):
        window = jnp.where(t >= n, jnp.int32(2 ** (n + 1)), window)
    position = s * seq + 1 + lax.broadcasted_iota(jnp.int32, (seq, GD), 0)
    divisor = jnp.minimum(position, window).astype(F32)
    pooled = (window_sum / divisor - values).astype(BF)
    product = jnp.dot(pooled, gmap[0], preferred_element_type=F32)
    piece[...] = (product * scale[...].astype(F32)).astype(BF).reshape(T, R, GD)

    def piece_copy(j):
        q = lax.rem(t + j, T)
        return remote(piece.at[q], gout.at[t], pc_s.at[0], pc_r.at[0], tp=q)

    for j in range(1, T):
        piece_copy(j).start()
    for k in range(1, H):
        o_far(k, NC - 1).start()
    gout[t] = piece[t]
    for c in C:
        opj[c, t] = oproj[:, cut(c)]

    slots = S * SL
    slot_iota = lax.broadcasted_iota(jnp.int32, (slots, R), 0).astype(F32)
    place = jnp.where((tgt_row[0] == slot_iota) | (tgt_row[1] == slot_iota), 1.0, 0.0).astype(BF)

    def z_copy(e, c):
        return remote(stage.at[c, e], inbox.at[s, c, t], z_s.at[0], z_r.at[s, c], sp=e)

    def z_arrival(i, c):
        return remote(stage.at[c, i], inbox.at[i, c, t], z_s.at[0], z_r.at[i, c], sp=i)

    def far_copy(i, k, c):
        block = inbox.at[i, c, t]
        return remote(block, block, f_s.at[k - 1], f_r.at[i, k - 1, c], tp=up(k))

    def near_copy(i, k, c):
        block = inbox.at[i, c, down(t, k)]
        return remote(block, block, n_s.at[0], n_r.at[i], tp=near)

    def r_copy(e, q, n):
        return remote(rsend.at[e], rin.at[s, t], rr_s.at[n], rr_r.at[s], sp=e, tp=q)

    def whole(ref, ss, rs):
        return remote(ref, ref, ss, rs, tp=near)

    def p_near(i, k, c):
        return remote(
            pbuf.at[i, c, down(near, k)], rbuf.at[i, c, k], pn_s.at[0], pn_r.at[i, c], tp=near
        )

    def p_far(i, k, c):
        q = down(t, k)
        return remote(
            pbuf.at[i, c, q], fbuf.at[i, k - 1, c], pf_s.at[k - 1], pf_r.at[i, k - 1, c], tp=q
        )

    def back(i, c):
        return remote(fin.at[i, c], ret.at[c, s], rz_s.at[0], rz_r.at[c], sp=i)

    def push(i, c):
        for k in range(1, H):
            far_copy(i, k, c).start()
        near_copy(i, 0, c).start()

    def fwd(p, c):
        i = visit(s, p, S)
        z_arrival(i, c).wait_recv()
        push(i, c)

    def relay(p, c):
        i = visit(s, p, S)
        for k in range(1, H):
            far_copy(i, k, c).wait_recv()
            near_copy(i, k, c).start()

    def ready(p):
        i = visit(s, p, S)
        whole(rbuf.at[i], n_s.at[0], n_r.at[i]).wait_recv()

        @pl.when(i != s)
        def _():
            whole(rin.at[i], rr_s.at[0], rr_r.at[i]).wait_recv()

        @pl.when(i == s)
        def _():
            whole(rin.at[i, pl.ds(0, T - 1)], rr_s.at[0], rr_r.at[i]).wait_recv()

    NT = 256 if (2 * F) % 256 == 0 else 128
    DT = 512
    GN = 2 * F // NT

    def hidden(p, lo, hi):
        i = visit(s, p, S)

        def one(n):
            cols = pl.ds(pl.multiple_of(n * NT, NT), NT)
            total = None
            for c in C:
                x = inbox[i, c].reshape(T * SL, DC)
                y = jnp.dot(x, wgu_v[cut(c), cols], preferred_element_type=F32)
                total = y if total is None else total + y
            acc[:, cols] = total

        for n in range(lo, hi):
            one(n)

    def gated(p):
        i = visit(s, p, S)
        spot = lax.broadcasted_iota(jnp.int32, (SL, 128), 0) == lax.broadcasted_iota(
            jnp.int32, (SL, 128), 1
        )
        for q in range(T):
            rows = slice(q * SL, (q + 1) * SL)
            r = jnp.sum(jnp.where(spot, rin[i, q], 0.0), axis=1, keepdims=True)
            gate = acc[rows, :F] * r
            hid[rows] = (gate / (1.0 + jnp.exp(-gate)) * (acc[rows, F:] * r)).astype(BF)

    def lower(p, c):
        i = visit(s, p, S)

        for n in range(DC // DT):
            y = jnp.dot(
                hid[...], wd_v[:, c * DC + n * DT : c * DC + (n + 1) * DT],
                preferred_element_type=F32,
            )
            pbuf[i, c, :, :, n * DT : (n + 1) * DT] = y.astype(BF).reshape(T, SL, DT)

        for k in range(H):
            p_near(i, k, c).start()

    def pair(p, c):
        i = visit(s, p, S)
        whole(rbuf.at[i, c], pn_s.at[0], pn_r.at[i, c]).wait_recv()
        for k in range(1, H):
            q = down(t, k)
            pbuf[i, c, q] = (pbuf[i, c, q].astype(F32) + rbuf[i, c, k].astype(F32)).astype(BF)
            p_far(i, k, c).start()

    def finish(p, c):
        i = visit(s, p, S)
        value = pbuf[i, c, t].astype(F32) + rbuf[i, c, 0].astype(F32)
        for k in range(1, H):
            p_far(i, k, c).wait_recv()
            value = value + fbuf[i, k - 1, c].astype(F32)
        return i, value.astype(BF)

    def send_back(p, c):
        i, value = finish(p, c)
        fin[i, c] = value
        back(i, c).start()

    def only(where, act, p, *c):
        @pl.when(where)
        def _():
            for n in c:
                act(p, n)

    def mix_part(c, wide, square):
        whole(opj.at[c, pl.ds(0, H)], on_s.at[0], on_r.at[c]).wait_recv()
        total = jnp.dot(wide, opj[c].reshape(T * GD, DC), preferred_element_type=F32)
        mixed = (resid[:, cut(c)].astype(F32) + total).astype(BF)
        mixed_v[:, cut(c)] = mixed
        residual = mixed.astype(F32)
        cast = (residual * gain[cut(c)].astype(F32).reshape(1, DC)).astype(BF)
        stage[c] = jnp.dot(place, cast, preferred_element_type=F32).astype(BF).reshape(S, SL, DC)
        inbox[s, c, t] = stage[c, s]

        z_copy(sends(s, 1, S), c).start()

        @pl.when(inner)
        def _():
            z_copy(sends(s, 2, S), c).start()

        push(s, c)
        return square + jnp.sum(residual * residual, axis=1, keepdims=True)

    square = jnp.zeros((R, 1), F32)
    o_spread(0)
    o_spread(1)
    for c in range(2, NC):
        o_pass(c - 2)
        o_spread(c)
    whole(gout.at[pl.ds(0, T - 1)], pc_s.at[0], pc_r.at[0]).wait_recv()
    wide = jnp.concatenate([gout[q] for q in range(T)], axis=1)
    for c in C:
        square = mix_part(c, wide, square)
        if c + 2 < NC:
            o_pass(c + NC - 2)
    unit = lax.rsqrt(square * (1.0 / D) + norm_eps)

    @pl.loop(0, S)
    def _(e):
        lane = (lax.broadcasted_iota(jnp.int32, (R, 128), 1) + e * SL).astype(F32)
        inside = lax.broadcasted_iota(jnp.int32, (R, 128), 1) < SL
        mine = ((tgt_col[0] == lane) | (tgt_col[1] == lane)) & inside
        rsend[e] = jnp.sum(jnp.where(mine, unit, 0.0), axis=0, keepdims=True)

    rin[s, t] = rsend[s]

    @pl.loop(1, T)
    def _(j):
        r_copy(s, lax.rem(t + j, T), 0).start()

    @pl.loop(0, (S - 1) * T)
    def _(j):
        r_copy(lax.rem(s + 1 + j // T, S), lax.rem(j, T), 1).start()

    @pl.loop(jnp.where(inner, 3, 2), S)
    def _(j):
        for c in C:
            z_copy(sends(s, j, S), c).start()

    for load in loads:
        load.wait()

    if S == 4:
        edge = (s == 0) | (s == S - 1)
        relay(0, 0)
        fwd(1, 0)
        relay(0, 1)
        fwd(1, 1)
        relay(0, 2)
        fwd(1, 2)
        relay(0, 3)
        ready(0)
        hidden(0, 0, 3)
        fwd(1, 3)
        relay(1, 0)
        hidden(0, 3, 5)
        hidden(0, 5, 7)
        relay(1, 1)
        fwd(2, 0)
        gated(0)
        lower(0, 0)
        relay(1, 2)
        lower(0, 1)
        fwd(2, 1)
        lower(0, 2)
        lower(0, 3)
        fwd(2, 2)
        relay(1, 3)
        ready(1)
        hidden(1, 0, 3)
        fwd(2, 3)
        only(inner, pair, 0, 0)
        relay(2, 0)
        hidden(1, 3, 5)
        relay(2, 1)
        hidden(1, 5, 7)
        only(edge, fwd, 3, 0)
        gated(1)
        relay(2, 2)
        lower(1, 0)
        only(edge, fwd, 3, 1)
        lower(1, 1)
        lower(1, 2)
        only(inner, pair, 1, 0)
        relay(2, 3)
        only(edge, fwd, 3, 2)
        lower(1, 3)
        only(inner, pair, 1, 1)
        only(edge, fwd, 3, 3)
        only(edge, pair, 1, 0)
        ready(2)
        only(inner, pair, 1, 2)
        hidden(2, 0, 3)
        only(inner, pair, 1, 3)
        only(inner, fwd, 3, 0)
        only(edge, relay, 3, 0)
        hidden(2, 3, 5)
        only(edge, relay, 3, 1)
        only(inner, fwd, 3, 1)
        only(inner, send_back, 1, 0)
        hidden(2, 5, 7)
        only(inner, fwd, 3, 2)
        gated(2)
        only(edge, relay, 3, 2)
        only(inner, send_back, 1, 1)
        lower(2, 0)
        only(inner, fwd, 3, 3)
        lower(2, 1)
        only(edge, pair, 2, 0)
        only(inner, send_back, 1, 2)
        lower(2, 2)
        only(edge, pair, 2, 1)
        only(edge, relay, 3, 3)
        lower(2, 3)
        only(inner, send_back, 1, 3)
        only(edge, pair, 2, 2, 3)
        only(edge, pair, 1, 1)
        only(inner, pair, 2, 0, 1, 2, 3)
        only(inner, pair, 0, 1)
        only(inner, relay, 3, 0, 1, 2, 3)
        ready(3)
        hidden(3, 0, 3)
        only(edge, send_back, 1, 0)
        only(edge, send_back, 2, 0)
        hidden(3, 3, 5)
        only(edge, send_back, 2, 1)
        only(inner, send_back, 2, 0)
        hidden(3, 5, 7)
        gated(3)
        only(edge, send_back, 2, 2)
        only(inner, send_back, 2, 1)
        lower(3, 0)
        lower(3, 1)
        lower(3, 2)
        pair(3, 0)
        pair(3, 1)
        only(inner, send_back, 2, 2)
        lower(3, 3)
        only(edge, send_back, 2, 3)
        pair(3, 2)
        pair(3, 3)
        only(edge, pair, 1, 2, 3)
        only(edge, pair, 0, 0, 1)
        pair(0, 2)
        pair(0, 3)
        only(inner, send_back, 2, 3)
        only(edge, send_back, 1, 1)
        send_back(3, 0)
        send_back(3, 1)
        send_back(3, 2)
        send_back(3, 3)
        only(edge, send_back, 1, 2, 3)
    else:
        @pl.loop(0, S + 1)
        def _(j):
            @pl.when(j < S)
            def _():
                for c in C:
                    relay(j, c)

            @pl.when(j + 1 < S)
            def _():
                for c in C:
                    fwd(j + 1, c)

            @pl.when(j > 1)
            def _():
                for c in C:
                    pair(j - 1, c)

            @pl.when(j < S)
            def _():
                ready(j)
                hidden(j, 0, GN)
                gated(j)
                for c in C:
                    lower(j, c)

            @pl.when(j > 1)
            def _():
                for c in C:
                    send_back(j - 1, c)

        for c in C:
            pair(0, c)

    lanes = lax.broadcasted_iota(jnp.int32, (R, slots), 1).astype(F32)
    pick = [jnp.where(tgt_col[k] == lanes, 1.0, 0.0).astype(BF) for k in range(2)]

    for c in C:
        _, value = finish(0, c)
        ret[c, s] = value
        whole(ret.at[c, pl.ds(0, S - 1)], rz_s.at[0], rz_r.at[c]).wait_recv()

        flat = ret[c].reshape(slots, DC)
        total = mixed_v[:, cut(c)].astype(F32)
        picked = [
            weight_col[k] * jnp.dot(pick[k], flat, preferred_element_type=F32) for k in range(2)
        ]
        out[:, cut(c)] = (total + (picked[0] + picked[1])).astype(BF)
        pltpu.make_async_copy(out.at[:, cut(c)], out_h.at[:, cut(c)], w_sem.at[3]).start()

    rim_copy.wait_send()
    half = opj.at[:, 0, pl.ds(0, GH)]
    for k in range(1, H):
        whole(half, ox_s.at[k - 1], ox_r.at[0, 0]).wait_send()
        for j in range(1, G):
            whole(half, oy_s.at[k - 1, j - 1], oy_r.at[0, 0, 0]).wait_send()
        whole(fin, f_s.at[k - 1], f_r.at[0, 0, 0]).wait_send()
        whole(fin, pf_s.at[k - 1], pf_r.at[0, 0, 0]).wait_send()
    whole(opj.at[:, pl.ds(0, H)], on_s.at[0], on_r.at[0]).wait_send()
    whole(piece.at[pl.ds(0, T - 1)], pc_s.at[0], pc_r.at[0]).wait_send()
    whole(rbuf, n_s.at[0], n_r.at[0]).wait_send()
    whole(rbuf, pn_s.at[0], pn_r.at[0, 0]).wait_send()
    others = fin.at[pl.ds(0, S - 1)]
    whole(others, z_s.at[0], z_r.at[0, 0]).wait_send()
    whole(others, rz_s.at[0], rz_r.at[0]).wait_send()
    whole(rin.at[0, pl.ds(0, T - 1)], rr_s.at[0], rr_r.at[0]).wait_send()
    whole(rin.at[pl.ds(0, S - 1)], rr_s.at[1], rr_r.at[0]).wait_send()
    pltpu.make_async_copy(out, out_h, w_sem.at[3]).wait()


def local(
    resid, pool_input, group_map, pool_scale, out_proj, norm_gain, routes, route_weight,
    expert_gate, expert_up, expert_down,
):
    G, S, T = lax.axis_size("grp"), lax.axis_size("sp"), lax.axis_size("tp")
    R, D = resid.shape
    H = T // 2
    top = routes.shape[1]
    experts = S * expert_gate.shape[0]
    room = max(2, 5 * R * top // (4 * experts))
    SL = -(-room // 16) * 16
    F = expert_down.shape[1]
    GD = group_map.shape[1]
    NC = 4
    DC = D // NC
    hbm = pl.BlockSpec(memory_space=pl.ANY)
    dma = lambda *n: pltpu.SemaphoreType.DMA(n)
    buf = lambda *n: pltpu.VMEM(n, BF)
    return pl.pallas_call(
        functools.partial(kernel, G, S, T, R, SL, NC),
        out_shape=jax.ShapeDtypeStruct((R, D), BF),
        in_specs=[hbm] * 11,
        out_specs=hbm,
        scratch_shapes=[
            buf(GD, D), buf(pool_input.shape[0], GD), buf(R, D), buf(1, GD, GD), buf(1, GD), buf(D),
            pltpu.VMEM((top, R), jnp.int32), pltpu.VMEM((top, R), F32), buf(R, D),
            buf(D, 2 * F), buf(F, D), buf(NC, T, GD, DC), buf(RIM, GD), buf(T, R, GD),
            buf(T, R, GD),
            buf(NC, S, SL, DC), buf(S, NC, T, SL, DC), buf(S, NC, T, SL, DC),
            buf(S, NC, H, SL, DC), buf(S, H - 1, NC, SL, DC), buf(S, NC, SL, DC),
            buf(NC, S, SL, DC),
            pltpu.VMEM((T * SL, 2 * F), F32), buf(T * SL, F), buf(R, D),
            pltpu.VMEM((S, 1, 128), F32), pltpu.VMEM((S, T, 1, 128), F32),
            dma(4), dma(8), dma(H - 1), dma(H - 1, NC), dma(H - 1, G - 1), dma(H - 1, G - 1, NC),
            dma(1), dma(NC), dma(1), dma(1), dma(1), dma(1),
            dma(1), dma(S, NC), dma(H - 1), dma(S, H - 1, NC), dma(1), dma(S),
            dma(1), dma(S, NC), dma(H - 1), dma(S, H - 1, NC), dma(1), dma(NC), dma(2), dma(S),
        ],
        compiler_params=pltpu.CompilerParams(
            collective_id=0, has_side_effects=True, vmem_limit_bytes=63 * 1024 * 1024
        ),
    )(
        resid, pool_input, group_map, pool_scale.reshape(1, -1), out_proj,
        norm_gain, routes.T, route_weight.T,
        expert_gate[0], expert_up[0], expert_down[0],
    )


def solution(mesh):
    return jax.shard_map(
        local,
        mesh=mesh,
        in_specs=(
            P(("grp", "sp", "tp"), None),
            P(("grp", "sp"), "tp"),
            P("tp", None, None),
            P("tp"),
            P("tp", None),
            P(),
            P(("grp", "sp", "tp"), None),
            P(("grp", "sp", "tp"), None),
            P("sp", None, "tp"),
            P("sp", None, "tp"),
            P("sp", "tp", None),
        ),
        out_specs=P(("grp", "sp", "tp"), None),
        check_vma=False,
    )
```
